32 devices in a mesh: kv: 16 (over z, y, x), tp: 2 (over core).
Axes of the slice: x: 2, y: 2, z: 4, core: 2. Of those that a mesh axis runs over, the one named last changes fastest.
Arguments:
- tokens: bfloat16 [160, 3, 2048], P('kv', None, 'tp'), may hold values from -6 to 6
- norm_gain: float32 [2048], replicated, may hold values from 0.1 to 1.9
- w_query: bfloat16 [2048, 1024], P('kv', 'tp'), may hold values from -0.125 to 0.125
- w_key: bfloat16 [2048, 1024], P('kv', 'tp'), may hold values from -0.125 to 0.125
- w_value: bfloat16 [2048, 2048], P('kv', 'tp'), may hold values from -0.125 to 0.125
- w_igate: bfloat16 [2048, 8], replicated, may hold values from -0.125 to 0.125
- w_fgate: bfloat16 [2048, 8], replicated, may hold values from -0.125 to 0.125
- igate_bias: float32 [8], replicated, may hold values from -5 to -2
- fgate_bias: float32 [8], replicated, may hold values from 0.5 to 4
- prev_keys: bfloat16 [160, 3, 1024], P('kv', None, 'tp'), may hold values from -6 to 6
- prev_values: bfloat16 [160, 3, 2048], P('kv', None, 'tp'), may hold values from -6 to 6
- prev_igate: float32 [160, 3, 8], P('kv', None, 'tp'), may hold values from -4 to 0
- prev_logf: float32 [160, 3, 8], P('kv', None, 'tp'), may hold values from -0.6 to -0.02
- accepted: int32 [160], P('kv'), may hold values from 0 to 3
- state_mem: float32 [160, 8, 128, 256], P('kv', 'tp'), may hold values from -2 to 2
- state_norm: float32 [160, 8, 128], P('kv', 'tp'), may hold values from -2 to 2
- state_max: float32 [160, 8], P('kv', 'tp'), may hold values from -3 to 0
Outputs:
- readout: bfloat16 [160, 3, 2048], P('kv', None, 'tp')
- base_mem: float32 [160, 8, 128, 256], P('kv', 'tp')
- base_norm: float32 [160, 8, 128], P('kv', 'tp')
- base_max: float32 [160, 8], P('kv', 'tp')
The draws below stay inside these ranges and needn't reach their ends.
Inputs may be any that keep to these rules, and one draw needn't show every extreme that they name: Proposal j of a sequence is live when j < accepted of that sequence.
All inputs are finite; a program needn't handle non-finite values.
Results may differ from the reference program's by a relative error of at most 0.0073.
Values may be sent and summed in bfloat16 or wider, within the bound.
A program may use at most 64 MiB of HBM per device.

```python
import jax
import jax.numpy as jnp
from jax import lax

D = 2048
HEADS = 8
DK = 128
DV = 256
PROPOSALS = 3
SEQS = 160


def draw_state_max(key, part):
    first = jax.random.fold_in(key, 0)
    settled = jax.random.uniform(first, (SEQS, HEADS), jnp.float32, -3.0, 0.0)
    return settled


def set_ends(values, rng, low, top_value):
    place = [jax.random.randint(jax.random.fold_in(rng, axis), (), 0, length) for axis, length in enumerate(values.shape)]
    longest = values.shape.index(max(values.shape))
    beside = place[:longest] + [(place[longest] + 1) % values.shape[longest]] + place[longest + 1:]
    return values.at[tuple(place)].set(low).at[tuple(beside)].set(top_value)


def block_levels(rng, shape, shards, least, largest):
    level, own = 1.0, jax.random.fold_in(rng, 6)
    for position, shards_of in shards:
        steps = jnp.exp(jax.random.uniform(jax.random.fold_in(own, position), (shards_of,), jnp.float32, least / len(shards), largest / len(shards)))
        level = level * jnp.repeat(steps, shape[position] // shards_of).reshape([-1 if axis == position else 1 for axis in range(len(shape))])
    return level


def gaussian(own_key, extent, spread, bound, pieces=(), held_as=jnp.bfloat16):
    values = jax.random.normal(own_key, extent, jnp.float32) * spread
    if len(pieces) > 0:
        values = block_levels(own_key, extent, pieces, -0.22, 0.18) * values
    return jnp.clip(values, min=-bound, max=bound).astype(held_as)


def setup_inputs(seed: int = 0) -> dict:
    arg_keys = jax.random.split(jax.random.key(seed), 18)
    return {
        "tokens": gaussian(arg_keys[0], (SEQS, PROPOSALS, D), 1.0, 6.0, ((0, 16), (2, 2))),
        "norm_gain": jnp.clip(1.0 + 0.18 * jax.random.normal(arg_keys[1], (D,), jnp.float32), 0.1, 1.9),
        "w_query": gaussian(arg_keys[2], (D, HEADS * DK), D ** -0.5, 0.125, ((0, 16), (1, 2))),
        "w_key": gaussian(arg_keys[3], (D, HEADS * DK), D ** -0.5, 0.125, ((0, 16), (1, 2))),
        "w_value": gaussian(arg_keys[4], (D, HEADS * DV), D ** -0.5, 0.125, ((0, 16), (1, 2))),
        "w_igate": gaussian(arg_keys[5], (D, HEADS), D ** -0.5, 0.125),
        "w_fgate": gaussian(arg_keys[6], (D, HEADS), D ** -0.5, 0.125),
        "igate_bias": jnp.clip(jax.random.uniform(arg_keys[7], (HEADS,), jnp.float32, -5.0, -2.0), -5.0, -2.0),
        "fgate_bias": jnp.clip(jax.random.uniform(arg_keys[8], (HEADS,), jnp.float32, 0.5, 4.0), 0.5, 4.0),
        "prev_keys": gaussian(arg_keys[9], (SEQS, PROPOSALS, HEADS * DK), 1.0, 6.0, ((0, 16), (2, 2))),
        "prev_values": gaussian(arg_keys[10], (SEQS, PROPOSALS, HEADS * DV), 1.0, 6.0, ((0, 16), (2, 2))),
        "prev_igate": jnp.clip(-4.0 + 4.0 * jax.random.uniform(arg_keys[11], (SEQS, PROPOSALS, HEADS), jnp.float32) ** block_levels(arg_keys[11], (SEQS, PROPOSALS, HEADS), ((0, 16), (2, 2)), -0.2, 0.2), -4.0, 0.0),
        "prev_logf": jnp.clip(-0.6 + 0.58000002 * jax.random.uniform(arg_keys[12], (SEQS, PROPOSALS, HEADS), jnp.float32) ** block_levels(arg_keys[12], (SEQS, PROPOSALS, HEADS), ((0, 16), (2, 2)), -0.2, 0.2), -0.6, -0.02),
        "accepted": set_ends(jax.random.randint(arg_keys[13], (SEQS,), 0, PROPOSALS + 1), jax.random.fold_in(arg_keys[13], 1), 0, PROPOSALS).astype(jnp.int32),
        "state_mem": gaussian(arg_keys[14], (SEQS, HEADS, DK, DV), 0.3, 2.0, ((0, 16), (1, 2)), jnp.float32),
        "state_norm": gaussian(arg_keys[15], (SEQS, HEADS, DK), 0.3, 2.0, ((0, 16), (1, 2)), jnp.float32),
        "state_max": draw_state_max(jax.random.fold_in(arg_keys[17], 71), 0),
    }


epsilon = 1e-06
highest = lax.Precision.HIGHEST

def fold_accepted(state_mem, state_norm, state_max, key_rows, value_rows, in_gate, log_forget, accepted):
    length = key_rows.shape[1]
    live_mask = (jnp.arange(length, dtype=jnp.int32)[None, :] < accepted[:, None])[:, :, None]
    forget_live = jnp.where(live_mask, log_forget, 0.0)
    cumulative = jnp.cumsum(forget_live, axis=1)
    totals = cumulative[:, -1]
    weight_log = jnp.where(live_mask, totals[:, None] - cumulative + in_gate, -jnp.inf)
    base_max = jnp.maximum(totals + state_max, lax.optimization_barrier(jnp.max(weight_log, axis=1)))
    carry_weight = jnp.exp(totals + state_max - base_max)
    weights = jnp.exp(weight_log - base_max[:, None])
    base_mem = carry_weight[..., None, None] * state_mem + jnp.einsum('sph,sphd,sphv->shdv', weights, key_rows, value_rows, precision=highest)
    base_norm = carry_weight[..., None] * state_norm + jnp.einsum('sph,sphd->shd', weights, key_rows, precision=highest)
    return (base_mem, base_norm, base_max)

def readout_block(base_mem, base_norm, base_max, query_rows, key_rows, value_rows, in_gate, log_forget):
    length = query_rows.shape[1]
    cumulative = jnp.cumsum(log_forget, axis=1)
    causal = jnp.arange(length, dtype=jnp.int32)[:, None] >= jnp.arange(length, dtype=jnp.int32)[None, :]
    within_log = cumulative[:, :, None, :] - cumulative[:, None, :, :] + in_gate[:, None, :, :]
    within_log = jnp.where(causal[None, :, :, None], within_log, -jnp.inf)
    carried_log = cumulative + base_max[:, None, :]
    top_log = jnp.maximum(carried_log, lax.optimization_barrier(jnp.max(within_log, axis=2)))
    scores = jnp.einsum('sthd,suhd->stuh', query_rows, key_rows, precision=highest) * jnp.exp(within_log - top_log[:, :, None, :])
    carried_weight = jnp.exp(carried_log - top_log)
    numerator = jnp.einsum('stuh,suhv->sthv', scores, value_rows, precision=highest) + carried_weight[..., None] * jnp.einsum('sthd,shdv->sthv', query_rows, base_mem, precision=highest)
    denominator = lax.optimization_barrier(jnp.sum(scores, axis=2)) + carried_weight * jnp.einsum('sthd,shd->sth', query_rows, base_norm, precision=highest)
    return numerator / jnp.maximum(jnp.abs(denominator), jnp.exp(-top_log))[..., None]

def reference(tokens, norm_gain, w_query, w_key, w_value, w_igate, w_fgate, igate_bias, fgate_bias, prev_keys, prev_values, prev_igate, prev_logf, accepted, state_mem, state_norm, state_max):
    seq_count, length, model_width = tokens.shape
    head_count = igate_bias.shape[0]
    key_width = state_mem.shape[2]
    value_width = state_mem.shape[3]
    key_scale = key_width ** (-0.5)
    flattened = tokens.reshape(seq_count * length, model_width).astype(jnp.float32)
    normed = (flattened * lax.rsqrt(lax.optimization_barrier(jnp.mean(flattened * flattened, axis=-1, keepdims=True)) + epsilon) * norm_gain).astype(jnp.bfloat16)
    query_rows = jnp.dot(normed, w_query, preferred_element_type=jnp.float32).astype(jnp.bfloat16)
    key_rows = jnp.dot(normed, w_key, preferred_element_type=jnp.float32).astype(jnp.bfloat16)
    value_rows = jnp.dot(normed, w_value, preferred_element_type=jnp.float32).astype(jnp.bfloat16)
    in_gate = jnp.dot(normed, w_igate, preferred_element_type=jnp.float32) + igate_bias
    log_forget = jax.nn.log_sigmoid(jnp.dot(normed, w_fgate, preferred_element_type=jnp.float32) + fgate_bias)

    def split_heads(matrix, last_width):
        return matrix.astype(jnp.float32).reshape(seq_count, length, head_count, last_width)
    base_mem, base_norm, base_max = fold_accepted(state_mem, state_norm, state_max, split_heads(prev_keys, key_width) * key_scale, split_heads(prev_values, value_width), prev_igate, prev_logf, accepted)
    hidden = readout_block(base_mem, base_norm, base_max, split_heads(query_rows, key_width), split_heads(key_rows, key_width) * key_scale, split_heads(value_rows, value_width), in_gate.reshape(seq_count, length, head_count), log_forget.reshape(seq_count, length, head_count))
    readout = hidden.reshape(seq_count, length, head_count * value_width).astype(jnp.bfloat16)
    return (readout, base_mem, base_norm, base_max)
```

```python
import functools

import jax
import jax.numpy as jnp
from jax import lax
from jax.experimental import pallas as pl
from jax.experimental.pallas import tpu as pltpu
from jax.sharding import PartitionSpec as P

epsilon = 1e-06
highest = lax.Precision.HIGHEST


def factor(count):
    inner = 1
    while inner * inner * 4 <= count and count % (inner * 2) == 0:
        inner *= 2
    return count // inner, inner


def step_kernel(
    reduce_n,
    outer_n,
    inner_n,
    tp_n,
    tok_ref,
    wq_ref,
    wk_ref,
    wv_ref,
    mem_ref,
    *refs,
):
    small_n = 12
    hbm_small, refs = refs[:small_n], refs[small_n:]
    (out_ref, mem_out, norm_out, max_out), refs = refs[:4], refs[4:]
    vmem_small, refs = refs[:small_n], refs[small_n:]
    (
        gain_ref,
        wi_ref,
        wf_ref,
        bi_ref,
        bf_ref,
        keys_ref,
        values_ref,
        gate_ref,
        logf_ref,
        accepted_ref,
        norm_ref,
        max_ref,
    ) = vmem_small
    (
        xfull,
        xrows,
        krows,
        vrows,
        scaled,
        mem16,
        carried,
        nbuf,
        abuf,
        xall,
        wbuf,
        pbuf,
        own,
        sbuf,
        rbuf,
        tok_local,
        tok_send,
        tok_recv,
        a_send,
        a_recv,
        w_local,
        w_send,
        w_recv,
        fy_send,
        fx_send,
        fy_recv,
        fx_recv,
        p_send,
        p_recv,
        mem_sem,
        small_sem,
    ) = refs
    group_n = outer_n * inner_n
    chunks, rows_all, width = wbuf.shape
    depth = rows_all // group_n
    half = depth // 2
    seqs, length, part = tok_ref.shape
    rows = seqs * length
    heads, _, value_width = mem16.shape
    key_width = mem_ref.shape[2]
    key_scale = key_width ** (-0.5)
    stride = xall.shape[0] // reduce_n
    block = nbuf.shape[2]

    kv = lax.axis_index("kv")
    tp = lax.axis_index("tp")
    red, grp = kv // group_n, kv % group_n
    outer, inner = grp // inner_n, grp % inner_n

    def at_grp(index):
        return {"kv": red * group_n + index}

    x_peers = [outer * inner_n + (inner + d) % inner_n for d in range(1, inner_n)]
    y_peers = [((outer + d) % outer_n) * inner_n + inner for d in range(1, outer_n)]
    r_peers = [(red + d) % reduce_n for d in range(1, reduce_n)]
    t_peers = [(tp + d) % tp_n for d in range(1, tp_n)]

    barrier = pltpu.get_barrier_semaphore()
    targets = (
        [{"tp": t} for t in t_peers]
        + [at_grp(p) for p in x_peers + y_peers]
        + [{"kv": p * group_n + grp} for p in r_peers]
    )
    for target in targets:
        pl.semaphore_signal(barrier, inc=1, device_id=target, device_id_type=pl.DeviceIdType.MESH)

    def chunk_of(c):
        if c == 0:
            return wq_ref
        if c == 1:
            return wk_ref
        return wv_ref.at[:, pl.ds((c - 2) * width, width)]

    def slot(c, source, start=0, size=None):
        size = depth if size is None else size
        first = pl.multiple_of(source * depth + start, half)
        return wbuf.at[c, pl.ds(first, size), :]

    def remote(src, dst, send, recv, target):
        return pltpu.make_async_remote_copy(
            src_ref=src,
            dst_ref=dst,
            send_sem=send,
            recv_sem=recv,
            device_id=target,
            device_id_type=pl.DeviceIdType.MESH,
        )

    locals_ = [pltpu.make_async_copy(tok_ref, xfull.at[tp], tok_local)]
    for c in range(chunks):
        locals_.append(pltpu.make_async_copy(chunk_of(c), slot(c, grp), w_local.at[c]))
    for copy in locals_:
        copy.start()
    small = [
        pltpu.make_async_copy(src, dst, small_sem.at[i])
        for i, (src, dst) in enumerate(zip(hbm_small, vmem_small))
    ]
    for copy in small:
        copy.start()
    mem_copy = pltpu.make_async_copy(mem_ref, mem_out, mem_sem)
    mem_copy.start()
    for copy in locals_:
        copy.wait()
    pl.semaphore_wait(barrier, len(targets))

    sends = []

    def go(copy):
        copy.start()
        sends.append(copy)

    for i, t in enumerate(t_peers):
        go(remote(xfull.at[tp], xfull.at[tp], tok_send.at[i], tok_recv.at[tp], {"tp": t}))

    def direct(c):
        for i, p in enumerate(x_peers + y_peers):
            go(remote(slot(c, grp), slot(c, grp), w_send.at[c, i], w_recv.at[c, grp], at_grp(p)))

    direct(0)
    if chunks > 1:
        direct(1)

    for copy in small:
        copy.wait()

    row_seq = lax.broadcasted_iota(jnp.int32, (rows, seqs), 0) // length
    row_pos = lax.broadcasted_iota(jnp.int32, (rows, seqs), 0) % length
    belongs = row_seq == lax.broadcasted_iota(jnp.int32, (rows, seqs), 1)
    diagonal = lax.broadcasted_iota(jnp.int32, (seqs, seqs), 0) == lax.broadcasted_iota(
        jnp.int32, (seqs, seqs), 1
    )

    accepted = accepted_ref[...]
    summed = jnp.zeros((heads, seqs), jnp.float32)
    sums = []
    for j in range(length):
        summed = summed + jnp.where(j < accepted, logf_ref[j], 0.0)
        sums.append(summed)
    logs = [
        jnp.where(j < accepted, summed - sums[j] + gate_ref[j], -jnp.inf) for j in range(length)
    ]
    top_log = summed + max_ref[...]
    for log in logs:
        top_log = jnp.maximum(top_log, log)
    max_out[...] = top_log
    weights = [jnp.exp(log - top_log) for log in logs]
    keep = jnp.exp(summed + max_ref[...] - top_log)

    krows[...] = jnp.zeros_like(krows)
    vrows[...] = jnp.zeros_like(vrows)
    scaled[...] = jnp.zeros_like(scaled)
    for n in range(seqs):
        krows[n * length : (n + 1) * length] = keys_ref[n].astype(jnp.float32)
        vrows[n * length : (n + 1) * length] = values_ref[n].astype(jnp.float32)
    values = vrows[...].astype(jnp.bfloat16)
    values = jnp.concatenate([values, values], axis=0)
    lane_seq = lax.broadcasted_iota(jnp.int32, (key_width, 2 * stride), 1) % stride // length
    pick_seq = (
        lax.broadcasted_iota(jnp.int32, (seqs, 2 * stride), 1) % stride // length
        == lax.broadcasted_iota(jnp.int32, (seqs, 2 * stride), 0)
    ).astype(jnp.bfloat16)

    def fold(h):
        column = jnp.zeros((rows, seqs), jnp.float32)
        for j in range(length):
            column = column + jnp.where(belongs & (row_pos == j), weights[j][h : h + 1], 0.0)
        column = jnp.sum(column, axis=1, keepdims=True)
        keys = krows[:rows, h * key_width : (h + 1) * key_width] * key_scale * column
        high = keys.astype(jnp.bfloat16).astype(jnp.float32)
        scaled[h, :rows] = high
        scaled[h, stride : stride + rows] = keys - high
        block_keys = scaled[h]
        upright = block_keys.T
        mine = values[:, h * value_width : (h + 1) * value_width]
        for n in range(seqs):
            left = jnp.where(lane_seq == n, upright, 0.0).astype(jnp.bfloat16)
            update = jnp.dot(left, mine, preferred_element_type=jnp.float32)
            fresh = keep[h : h + 1, n : n + 1] * mem_out[n, h] + update
            mem_out[n, h] = fresh
            mem16[h, n * key_width : (n + 1) * key_width] = fresh.astype(jnp.bfloat16)
        carry = jnp.sum(jnp.where(diagonal, keep[h : h + 1], 0.0), axis=1, keepdims=True)
        added = jnp.dot(pick_seq, block_keys.astype(jnp.bfloat16), preferred_element_type=jnp.float32)
        norm_out[:, h, :] = carry * norm_ref[:, h, :] + added

    for t in t_peers:
        remote(tok_ref, xfull.at[t], tok_send.at[0], tok_recv.at[t], {"tp": t}).wait_recv()

    total = jnp.zeros((rows, 1), jnp.float32)
    for t in range(tp_n):
        for n in range(seqs):
            xrows[t, n * length : (n + 1) * length] = xfull[t, n].astype(jnp.float32)
        piece = xrows[t]
        total = total + jnp.sum(piece * piece, axis=1, keepdims=True)
    factor_rows = lax.rsqrt(total / (tp_n * part) + epsilon)
    step = min(block, part)
    for p in range(reduce_n * block // step):
        first = p * step
        piece = xrows[first // part, :, first % part : first % part + step]
        normed = (piece * factor_rows * gain_ref[:, first : first + step]).astype(jnp.bfloat16)
        nbuf[first // block, :, first % block : first % block + step] = normed

    for i, p in enumerate(r_peers):
        go(remote(nbuf.at[p], abuf.at[red], a_send.at[i], a_recv.at[red], {"kv": p * group_n + grp}))
    abuf[red] = nbuf[red]

    dims = (((1,), (1,)), ((), ()))
    gate_i = jnp.zeros((rows, wi_ref.shape[0]), jnp.float32)
    gate_f = jnp.zeros((rows, wf_ref.shape[0]), jnp.float32)
    for p in range(reduce_n):
        cols = slice(p * block, (p + 1) * block)
        piece = nbuf[p]
        gate_i += lax.dot_general(piece, wi_ref[:, cols], dims, preferred_element_type=jnp.float32)
        gate_f += lax.dot_general(piece, wf_ref[:, cols], dims, preferred_element_type=jnp.float32)
    gate_i = gate_i + bi_ref[...]
    gate_f = jax.nn.log_sigmoid(gate_f + bf_ref[...])
    row_id = lax.broadcasted_iota(jnp.int32, (rows, rows), 0)
    col_id = lax.broadcasted_iota(jnp.int32, (rows, rows), 1)
    causal = (row_id // length == col_id // length) & (col_id <= row_id)
    same = row_id == col_id
    head_id = lax.broadcasted_iota(jnp.int32, gate_i.shape, 1)

    def turned(column):
        return jnp.sum(jnp.where(same, column, 0.0), axis=0, keepdims=True)

    decays, tops, carries = [], [], []
    for h in range(heads):
        chosen = head_id == tp * heads + h
        in_gate = jnp.sum(jnp.where(chosen, gate_i, 0.0), axis=1, keepdims=True)
        log_forget = jnp.sum(jnp.where(chosen, gate_f, 0.0), axis=1, keepdims=True)
        running = jnp.sum(jnp.where(causal, turned(log_forget), 0.0), axis=1, keepdims=True)
        within = jnp.where(causal, running + turned(in_gate - running), -jnp.inf)
        base_max = jnp.sum(jnp.where(belongs, top_log[h : h + 1], 0.0), axis=1, keepdims=True)
        top = jnp.maximum(running + base_max, jnp.max(within, axis=1, keepdims=True))
        decays.append(jnp.exp(within - top) * key_scale)
        carries.append(jnp.exp(running + base_max - top))
        tops.append(jnp.exp(-top))

    xall[...] = jnp.zeros_like(xall)
    for p in r_peers:
        remote(nbuf.at[p], abuf.at[p], a_send.at[0], a_recv.at[p], {"kv": p * group_n + grp}).wait_recv()
    for p in range(reduce_n):
        xall[p * stride : p * stride + rows, :] = abuf[p]

    def relay(c):
        for i, p in enumerate(x_peers):
            remote(chunk_of(c), slot(c, p), w_send.at[c, 0], w_recv.at[c, p], at_grp(p)).wait_recv()
            for j, q in enumerate(y_peers):
                go(
                    remote(
                        slot(c, p, 0, half),
                        slot(c, p, 0, half),
                        fy_send.at[c, i, j],
                        fy_recv.at[c, p],
                        at_grp(q),
                    )
                )
        for j, q in enumerate(y_peers):
            remote(chunk_of(c), slot(c, q), w_send.at[c, 0], w_recv.at[c, q], at_grp(q)).wait_recv()
            for i, p in enumerate(x_peers):
                go(
                    remote(
                        slot(c, q, half, half),
                        slot(c, q, half, half),
                        fx_send.at[c, i, j],
                        fx_recv.at[c, q],
                        at_grp(p),
                    )
                )
        if c + 2 < chunks:
            direct(c + 2)

    def partial(c):
        for i in range(1, inner_n):
            for j in range(1, outer_n):
                source = ((outer + j) % outer_n) * inner_n + (inner + i) % inner_n
                for start, send, recv in ((0, fy_send, fy_recv), (half, fx_send, fx_recv)):
                    here = slot(c, source, start, half)
                    remote(here, here, send.at[c, 0, 0], recv.at[c, source], at_grp(source)).wait_recv()
        product = jnp.dot(xall[...], wbuf[c], preferred_element_type=jnp.float32)
        for p in range(reduce_n):
            piece = product[p * stride : p * stride + rows]
            pbuf[p] = piece
            sbuf[c, p] = piece.astype(jnp.bfloat16)
        own[c] = pbuf[red]
        for i, p in enumerate(r_peers):
            go(
                remote(
                    sbuf.at[c, p],
                    rbuf.at[c, red],
                    p_send.at[c, i],
                    p_recv.at[c, red],
                    {"kv": p * group_n + grp},
                )
            )

    def settle(c):
        total = own[c]
        for p in r_peers:
            remote(
                sbuf.at[c, p], rbuf.at[c, p], p_send.at[c, 0], p_recv.at[c, p], {"kv": p * group_n + grp}
            ).wait_recv()
            total = total + rbuf[c, p].astype(jnp.float32)
        return total.astype(jnp.bfloat16)

    kept = {}

    def finish(c):
        done = settle(c)
        if c == 0:
            kept["query"] = done
            seq_id = lax.broadcasted_iota(jnp.int32, (rows, key_width), 0) // length
            for h in range(heads):
                query = done[:, h * key_width : (h + 1) * key_width].astype(jnp.float32)
                spread = jnp.concatenate(
                    [jnp.where(seq_id == n, query, 0.0).astype(jnp.bfloat16) for n in range(seqs)],
                    axis=1,
                )
                held = jnp.dot(spread, mem16[h], preferred_element_type=jnp.float32)
                carried[h] = held * carries[h]
                against = lax.dot_general(
                    query, norm_out[:, h, :], dims, precision=highest,
                    preferred_element_type=jnp.float32,
                )
                kept["norm", h] = carries[h] * jnp.sum(
                    jnp.where(belongs, against, 0.0), axis=1, keepdims=True
                )
        elif c == 1:
            for h in range(heads):
                cols = slice(h * key_width, (h + 1) * key_width)
                scores = decays[h] * lax.dot_general(
                    kept["query"][:, cols], done[:, cols], dims, preferred_element_type=jnp.float32
                )
                den = jnp.sum(scores, axis=1, keepdims=True) + kept["norm", h]
                kept["scores", h] = scores
                kept["den", h] = jnp.maximum(jnp.abs(den), tops[h])
        else:
            wide = min(width, value_width)
            for i in range(width // wide):
                first = (c - 2) * width + i * wide
                h, sub = first // value_width, first % value_width
                scores = kept["scores", h]
                high = scores.astype(jnp.bfloat16)
                low = (scores - high.astype(jnp.float32)).astype(jnp.bfloat16)
                mine = done[:, i * wide : (i + 1) * wide]
                num = carried[h, :, sub : sub + wide]
                num = num + jnp.dot(high, mine, preferred_element_type=jnp.float32)
                num = num + jnp.dot(low, mine, preferred_element_type=jnp.float32)
                result = num / kept["den", h]
                for n in range(seqs):
                    out_ref[n, :, first : first + wide] = result[
                        n * length : (n + 1) * length
                    ].astype(jnp.bfloat16)

    for c in range(chunks + 2):
        if c < chunks:
            if c == 0:
                mem_copy.wait()
            relay(c)
            for h in range(c, heads, 2) if c < 2 else ():
                fold(h)
        if 1 <= c <= chunks:
            partial(c - 1)
        if c >= 2:
            finish(c - 2)
    for copy in sends:
        copy.wait_send()


def write_kernel(*refs):
    count = (len(refs) - 1) // 2
    sems = refs[-1]
    copies = []
    for src, dst in zip(refs[:count], refs[count : 2 * count]):
        if len(src.shape) == 4:
            for n in range(src.shape[0]):
                copies.append((src.at[n], dst.at[n]))
        else:
            copies.append((src, dst))
    copies = [pltpu.make_async_copy(s, d, sems.at[i]) for i, (s, d) in enumerate(copies)]
    for copy in copies:
        copy.start()
    for copy in copies:
        copy.wait()


def step(
    tokens,
    norm_gain,
    w_query,
    w_key,
    w_value,
    w_igate,
    w_fgate,
    igate_bias,
    fgate_bias,
    prev_keys,
    prev_values,
    prev_igate,
    prev_logf,
    accepted,
    state_mem,
    state_norm,
    state_max,
    kv_n,
    tp_n,
):
    seqs, length, part = tokens.shape
    rows = seqs * length
    heads, key_width, value_width = state_mem.shape[1:]
    depth, width = w_query.shape
    chunks = 2 + w_value.shape[1] // width
    reduce_n, group_n = factor(kv_n)
    outer_n, inner_n = factor(group_n)
    block = group_n * depth
    stride = -(-rows // 16) * 16
    dma = pltpu.SemaphoreType.DMA
    peers = max(1, outer_n + inner_n - 2)
    vmem = pl.BlockSpec(memory_space=pltpu.VMEM)
    hbm = pl.BlockSpec(memory_space=pl.ANY)
    small = (
        norm_gain.reshape(1, -1),
        w_igate.T,
        w_fgate.T,
        igate_bias.reshape(1, -1),
        fgate_bias.reshape(1, -1),
        prev_keys,
        prev_values,
        prev_igate.transpose(1, 2, 0),
        prev_logf.transpose(1, 2, 0),
        accepted.reshape(1, -1),
        state_norm,
        state_max.T,
    )
    results = (
        jax.ShapeDtypeStruct((seqs, length, heads * value_width), jnp.bfloat16),
        jax.ShapeDtypeStruct(state_mem.shape, jnp.float32),
        jax.ShapeDtypeStruct(state_norm.shape, jnp.float32),
        jax.ShapeDtypeStruct((heads, seqs), jnp.float32),
    )
    held = pl.pallas_call(
        functools.partial(step_kernel, reduce_n, outer_n, inner_n, tp_n),
        out_shape=results,
        in_specs=[hbm] * (5 + len(small)),
        out_specs=[vmem] * len(results),
        scratch_shapes=[pltpu.VMEM(x.shape, x.dtype) for x in small]
        + [
            pltpu.VMEM((tp_n, seqs, length, part), jnp.bfloat16),
            pltpu.VMEM((tp_n, rows, part), jnp.float32),
            pltpu.VMEM((stride, heads * key_width), jnp.float32),
            pltpu.VMEM((stride, heads * value_width), jnp.float32),
            pltpu.VMEM((heads, 2 * stride, key_width), jnp.float32),
            pltpu.VMEM((heads, seqs * key_width, value_width), jnp.bfloat16),
            pltpu.VMEM((heads, rows, value_width), jnp.float32),
            pltpu.VMEM((reduce_n, rows, block), jnp.bfloat16),
            pltpu.VMEM((reduce_n, rows, block), jnp.bfloat16),
            pltpu.VMEM((reduce_n * stride, block), jnp.bfloat16),
            pltpu.VMEM((chunks, block, width), jnp.bfloat16),
            pltpu.VMEM((reduce_n, rows, width), jnp.float32),
            pltpu.VMEM((chunks, rows, width), jnp.float32),
            pltpu.VMEM((chunks, reduce_n, rows, width), jnp.bfloat16),
            pltpu.VMEM((chunks, reduce_n, rows, width), jnp.bfloat16),
            dma,
            dma((tp_n,)),
            dma((tp_n,)),
            dma((reduce_n,)),
            dma((reduce_n,)),
            dma((chunks,)),
            dma((chunks, peers)),
            dma((chunks, group_n)),
            dma((chunks, inner_n, outer_n)),
            dma((chunks, inner_n, outer_n)),
            dma((chunks, group_n)),
            dma((chunks, group_n)),
            dma((chunks, reduce_n)),
            dma((chunks, reduce_n)),
            dma,
            dma((len(small),)),
        ],
        compiler_params=pltpu.CompilerParams(
            collective_id=0, has_side_effects=True, vmem_limit_bytes=40 * 2**20
        ),
        name="step",
    )(*(pltpu.with_memory_space_constraint(x, pltpu.HBM) for x in (tokens, w_query, w_key, w_value, state_mem) + small))
    return pl.pallas_call(
        write_kernel,
        out_shape=results,
        in_specs=[vmem] * len(results),
        out_specs=[hbm] * len(results),
        scratch_shapes=[dma((seqs + len(results),))],
        compiler_params=pltpu.CompilerParams(vmem_limit_bytes=8 * 2**20),
        name="write",
    )(*held)


def shards(kv_n, tp_n, *args):
    readout, base_mem, base_norm, base_max = step(*args, kv_n, tp_n)
    return (readout, base_mem, base_norm, base_max.T)


def solution(mesh):
    return jax.shard_map(
        functools.partial(shards, mesh.shape["kv"], mesh.shape["tp"]),
        mesh=mesh,
        in_specs=(
            P("kv", None, "tp"),
            P(),
            P("kv", "tp"),
            P("kv", "tp"),
            P("kv", "tp"),
            P(),
            P(),
            P(),
            P(),
            P("kv", None, "tp"),
            P("kv", None, "tp"),
            P("kv", None, "tp"),
            P("kv", None, "tp"),
            P("kv"),
            P("kv", "tp", None, None),
            P("kv", "tp", None),
            P("kv", "tp"),
        ),
        out_specs=(
            P("kv", None, "tp"),
            P("kv", "tp", None, None),
            P("kv", "tp", None),
            P("kv", "tp"),
        ),
        check_vma=False,
    )
```

```python
import functools

import jax
import jax.numpy as jnp
from jax import lax
from jax.experimental import pallas as pl
from jax.experimental.pallas import tpu as pltpu
from jax.sharding import PartitionSpec as P

epsilon = 1e-06
pool = 12
highest = lax.Precision.HIGHEST


def factor(count):
    inner = 1
    while inner * inner * 4 <= count and count % (inner * 2) == 0:
        inner *= 2
    return count // inner, inner


def step_kernel(
    reduce_n,
    outer_n,
    inner_n,
    tp_n,
    tok_ref,
    wq_ref,
    wk_ref,
    wv_ref,
    mem_ref,
    *refs,
):
    small_n = 12
    hbm_small, refs = refs[:small_n], refs[small_n:]
    (out_ref, mem_out, norm_out, max_out), refs = refs[:4], refs[4:]
    vmem_small, refs = refs[:small_n], refs[small_n:]
    (
        gain_ref,
        wi_ref,
        wf_ref,
        bi_ref,
        bf_ref,
        keys_ref,
        values_ref,
        gate_ref,
        logf_ref,
        accepted_ref,
        norm_ref,
        max_ref,
    ) = vmem_small
    (
        xfull,
        xrows,
        krows,
        vrows,
        scaled,
        mem16,
        carried,
        nbuf,
        abuf,
        xall,
        wbuf,
        own,
        sbuf,
        rbuf,
        tok_local,
        send_sem,
        tok_recv,
        a_recv,
        w_local,
        w_recv,
        f_recv,
        p_recv,
        mem_sem,
        small_sem,
        up_sem,
        down_sem,
    ) = refs
    group_n = outer_n * inner_n
    chunks, rows_all, width = wbuf.shape
    depth = rows_all // group_n
    half = depth // 2
    seqs, length, part = tok_ref.shape
    rows = seqs * length
    heads, _, value_width = mem16.shape
    key_width = mem_ref.shape[2]
    key_scale = key_width ** (-0.5)
    stride = xall.shape[0] // reduce_n
    block = nbuf.shape[2]

    kv = lax.axis_index("kv")
    tp = lax.axis_index("tp")
    red, grp = kv // group_n, kv % group_n
    outer, inner = grp // inner_n, grp % inner_n

    def at_grp(index):
        return {"kv": red * group_n + index}

    x_peers = [outer * inner_n + (inner + d) % inner_n for d in range(1, inner_n)]
    y_peers = [((outer + d) % outer_n) * inner_n + inner for d in range(1, outer_n)]
    t_peers = [(tp + d) % tp_n for d in range(1, tp_n)]
    x_back = [outer * inner_n + (inner + inner_n - d) % inner_n for d in range(1, inner_n)]
    y_back = [((outer + outer_n - d) % outer_n) * inner_n + inner for d in range(1, outer_n)]
    r_peers = [(red + d) % reduce_n for d in range(1, reduce_n)]
    r_back = [(red + reduce_n - d) % reduce_n for d in range(1, reduce_n)]
    t_back = [(tp + tp_n - d) % tp_n for d in range(1, tp_n)]

    barrier = pltpu.get_barrier_semaphore()
    targets = (
        [{"tp": t} for t in t_peers]
        + [at_grp(p) for p in x_peers + y_peers]
    )

    def signal(sem, target):
        pl.semaphore_signal(sem, inc=1, device_id=target, device_id_type=pl.DeviceIdType.MESH)

    def at_red(index):
        return {"kv": index * group_n + grp}

    for target in targets:
        signal(barrier, target)
    has_below, has_above = red > 0, red < reduce_n - 1
    if reduce_n > 1:
        pl.when(has_below)(lambda: signal(barrier, at_red(red - 1)))
        pl.when(has_above)(lambda: signal(barrier, at_red(red + 1)))

    def chunk_of(c):
        if c == 0:
            return wq_ref
        if c == 1:
            return wk_ref
        return wv_ref.at[:, pl.ds((c - 2) * width, width)]

    def slot(c, source, start=0, size=None):
        size = depth if size is None else size
        first = pl.multiple_of(source * depth + start, half)
        return wbuf.at[c, pl.ds(first, size), :]

    def remote(src, dst, send, recv, target):
        return pltpu.make_async_remote_copy(
            src_ref=src,
            dst_ref=dst,
            send_sem=send,
            recv_sem=recv,
            device_id=target,
            device_id_type=pl.DeviceIdType.MESH,
        )

    locals_ = [pltpu.make_async_copy(tok_ref, xfull.at[tp], tok_local)]
    for c in range(chunks):
        locals_.append(pltpu.make_async_copy(chunk_of(c), slot(c, grp), w_local.at[c]))
    for copy in locals_:
        copy.start()
    small = [
        pltpu.make_async_copy(src, dst, small_sem.at[i])
        for i, (src, dst) in enumerate(zip(hbm_small, vmem_small))
    ]
    for copy in small:
        copy.start()
    mem_copy = pltpu.make_async_copy(mem_ref, mem_out, mem_sem)
    mem_copy.start()
    for copy in locals_:
        copy.wait()
    greeted = len(targets)
    if reduce_n > 1:
        greeted = greeted + jnp.minimum(red, 1) + jnp.minimum(reduce_n - 1 - red, 1)
    pl.semaphore_wait(barrier, greeted)

    sends = []

    def go(src, dst, recv, target):
        count = len(sends)
        if count >= pool:
            sends[count - pool].wait_send()
        copy = remote(src, dst, send_sem.at[count % pool], recv, target)
        copy.start()
        sends.append(copy)

    for i, t in enumerate(t_peers):
        go(xfull.at[tp], xfull.at[tp], tok_recv.at[i], {"tp": t})

    def direct(c):
        for i, p in enumerate(x_peers + y_peers):
            go(slot(c, grp), slot(c, grp), w_recv.at[c, i], at_grp(p))

    direct(0)
    if chunks > 1:
        direct(1)

    if reduce_n > 2:
        last = reduce_n - 1
        pl.when(red == 1)(lambda: signal(up_sem, at_red(red + 1)))
        pl.when(red == last - 1)(lambda: signal(down_sem, at_red(red - 1)))
        pl.when(red >= 2)(lambda: pl.semaphore_wait(up_sem, 1))
        pl.when((red >= 2) & (red < last))(lambda: signal(up_sem, at_red(red + 1)))
        pl.when(red <= last - 2)(lambda: pl.semaphore_wait(down_sem, 1))
        pl.when((red <= last - 2) & (red > 0))(lambda: signal(down_sem, at_red(red - 1)))

    for i, t in enumerate(t_back):
        remote(xfull.at[t], xfull.at[t], send_sem.at[0], tok_recv.at[i], {"tp": t}).wait_recv()

    small[0].wait()
    total = jnp.zeros((rows, 1), jnp.float32)
    for t in range(tp_n):
        for n in range(seqs):
            xrows[t, n * length : (n + 1) * length] = xfull[t, n].astype(jnp.float32)
        piece = xrows[t]
        total = total + jnp.sum(piece * piece, axis=1, keepdims=True)
    factor_rows = lax.rsqrt(total / (tp_n * part) + epsilon)
    step = min(block, part)
    for p in range(reduce_n * block // step):
        first = p * step
        piece = xrows[first // part, :, first % part : first % part + step]
        normed = (piece * factor_rows * gain_ref[:, first : first + step]).astype(jnp.bfloat16)
        nbuf[first // block, :, first % block : first % block + step] = normed

    for i, p in enumerate(r_peers):
        go(nbuf.at[p], abuf.at[i], a_recv, {"kv": p * group_n + grp})

    for copy in small[1:]:
        copy.wait()

    row_seq = lax.broadcasted_iota(jnp.int32, (rows, seqs), 0) // length
    row_pos = lax.broadcasted_iota(jnp.int32, (rows, seqs), 0) % length
    belongs = row_seq == lax.broadcasted_iota(jnp.int32, (rows, seqs), 1)
    diagonal = lax.broadcasted_iota(jnp.int32, (seqs, seqs), 0) == lax.broadcasted_iota(
        jnp.int32, (seqs, seqs), 1
    )

    accepted = accepted_ref[...]
    summed = jnp.zeros((heads, seqs), jnp.float32)
    sums = []
    for j in range(length):
        summed = summed + jnp.where(j < accepted, logf_ref[j], 0.0)
        sums.append(summed)
    logs = [
        jnp.where(j < accepted, summed - sums[j] + gate_ref[j], -jnp.inf) for j in range(length)
    ]
    top_log = summed + max_ref[...]
    for log in logs:
        top_log = jnp.maximum(top_log, log)
    max_out[...] = top_log
    weights = [jnp.exp(log - top_log) for log in logs]
    keep = jnp.exp(summed + max_ref[...] - top_log)

    krows[...] = jnp.zeros_like(krows)
    vrows[...] = jnp.zeros_like(vrows)
    scaled[...] = jnp.zeros_like(scaled)
    for n in range(seqs):
        krows[n * length : (n + 1) * length] = keys_ref[n].astype(jnp.float32)
        vrows[n * length : (n + 1) * length] = values_ref[n].astype(jnp.float32)
    values = vrows[...].astype(jnp.bfloat16)
    values = jnp.concatenate([values, values], axis=0)
    lane_seq = lax.broadcasted_iota(jnp.int32, (key_width, 2 * stride), 1) % stride // length
    pick_seq = (
        lax.broadcasted_iota(jnp.int32, (seqs, 2 * stride), 1) % stride // length
        == lax.broadcasted_iota(jnp.int32, (seqs, 2 * stride), 0)
    ).astype(jnp.bfloat16)

    def fold(h):
        column = jnp.zeros((rows, seqs), jnp.float32)
        for j in range(length):
            column = column + jnp.where(belongs & (row_pos == j), weights[j][h : h + 1], 0.0)
        column = jnp.sum(column, axis=1, keepdims=True)
        keys = krows[:rows, h * key_width : (h + 1) * key_width] * key_scale * column
        high = keys.astype(jnp.bfloat16).astype(jnp.float32)
        scaled[h, :rows] = high
        scaled[h, stride : stride + rows] = keys - high
        block_keys = scaled[h]
        upright = block_keys.T
        mine = values[:, h * value_width : (h + 1) * value_width]
        for n in range(seqs):
            left = jnp.where(lane_seq == n, upright, 0.0).astype(jnp.bfloat16)
            update = jnp.dot(left, mine, preferred_element_type=jnp.float32)
            fresh = keep[h : h + 1, n : n + 1] * mem_out[n, h] + update
            mem_out[n, h] = fresh
            mem16[h, n * key_width : (n + 1) * key_width] = fresh.astype(jnp.bfloat16)
        carry = jnp.sum(jnp.where(diagonal, keep[h : h + 1], 0.0), axis=1, keepdims=True)
        added = jnp.dot(pick_seq, block_keys.astype(jnp.bfloat16), preferred_element_type=jnp.float32)
        norm_out[:, h, :] = carry * norm_ref[:, h, :] + added

    dims = (((1,), (1,)), ((), ()))
    gate_i = jnp.zeros((rows, wi_ref.shape[0]), jnp.float32)
    gate_f = jnp.zeros((rows, wf_ref.shape[0]), jnp.float32)
    for p in range(reduce_n):
        cols = slice(p * block, (p + 1) * block)
        piece = nbuf[p]
        gate_i += lax.dot_general(piece, wi_ref[:, cols], dims, preferred_element_type=jnp.float32)
        gate_f += lax.dot_general(piece, wf_ref[:, cols], dims, preferred_element_type=jnp.float32)
    gate_i = gate_i + bi_ref[...]
    gate_f = jax.nn.log_sigmoid(gate_f + bf_ref[...])
    row_id = lax.broadcasted_iota(jnp.int32, (rows, rows), 0)
    col_id = lax.broadcasted_iota(jnp.int32, (rows, rows), 1)
    causal = (row_id // length == col_id // length) & (col_id <= row_id)
    same = row_id == col_id
    head_id = lax.broadcasted_iota(jnp.int32, gate_i.shape, 1)

    def turned(column):
        return jnp.sum(jnp.where(same, column, 0.0), axis=0, keepdims=True)

    decays, tops, carries = [], [], []
    for h in range(heads):
        chosen = head_id == tp * heads + h
        in_gate = jnp.sum(jnp.where(chosen, gate_i, 0.0), axis=1, keepdims=True)
        log_forget = jnp.sum(jnp.where(chosen, gate_f, 0.0), axis=1, keepdims=True)
        running = jnp.sum(jnp.where(causal, turned(log_forget), 0.0), axis=1, keepdims=True)
        within = jnp.where(causal, running + turned(in_gate - running), -jnp.inf)
        base_max = jnp.sum(jnp.where(belongs, top_log[h : h + 1], 0.0), axis=1, keepdims=True)
        top = jnp.maximum(running + base_max, jnp.max(within, axis=1, keepdims=True))
        decays.append(jnp.exp(within - top) * key_scale)
        carries.append(jnp.exp(running + base_max - top))
        tops.append(jnp.exp(-top))

    def receive_rows():
        xall[...] = jnp.zeros_like(xall)
        xall[:rows, :] = nbuf[red]
        if reduce_n > 1:
            remote(abuf, abuf, send_sem.at[0], a_recv, {"kv": r_back[0] * group_n + grp}).wait_recv()
        for i in range(reduce_n - 1):
            xall[(i + 1) * stride : (i + 1) * stride + rows, :] = abuf[i]

    def relay(c):
        for i, p in enumerate(x_back):
            remote(slot(c, p), slot(c, p), send_sem.at[0], w_recv.at[c, i], at_grp(p)).wait_recv()
            for j, q in enumerate(y_peers):
                piece = slot(c, p, 0, half)
                go(piece, piece, f_recv.at[c, i, j], at_grp(q))
        for j, q in enumerate(y_back):
            k = len(x_back) + j
            remote(slot(c, q), slot(c, q), send_sem.at[0], w_recv.at[c, k], at_grp(q)).wait_recv()
            for i, p in enumerate(x_peers):
                piece = slot(c, q, half, half)
                go(piece, piece, f_recv.at[c, i, j], at_grp(p))
        if c + 2 < chunks:
            direct(c + 2)

    def partial(c):
        for i, p in enumerate(x_back):
            for j, q in enumerate(y_back):
                source = q - inner + p - outer * inner_n
                here = slot(c, source)
                remote(here, here, send_sem.at[0], f_recv.at[c, i, j], at_grp(source)).wait_recv()
        product = jnp.dot(xall[...], wbuf[c], preferred_element_type=jnp.float32)
        own[c] = product[:rows]
        for i, p in reversed(list(enumerate(r_back))):
            piece = product[(i + 1) * stride : (i + 1) * stride + rows]
            sbuf[c, i] = piece.astype(jnp.bfloat16)
            go(sbuf.at[c, i], rbuf.at[c, i], p_recv.at[c], {"kv": p * group_n + grp})

    def settle(c):
        total = own[c]
        if reduce_n > 1:
            here = rbuf.at[c]
            source = {"kv": r_back[0] * group_n + grp}
            remote(here, here, send_sem.at[0], p_recv.at[c], source).wait_recv()
        for i in range(reduce_n - 1):
            total = total + rbuf[c, i].astype(jnp.float32)
        return total.astype(jnp.bfloat16)

    kept = {}

    def finish(c):
        done = settle(c)
        if c == 0:
            kept["query"] = done
            seq_id = lax.broadcasted_iota(jnp.int32, (rows, key_width), 0) // length
            for h in range(heads):
                query = done[:, h * key_width : (h + 1) * key_width].astype(jnp.float32)
                spread = jnp.concatenate(
                    [jnp.where(seq_id == n, query, 0.0).astype(jnp.bfloat16) for n in range(seqs)],
                    axis=1,
                )
                held = jnp.dot(spread, mem16[h], preferred_element_type=jnp.float32)
                carried[h] = held * carries[h]
                against = lax.dot_general(
                    query, norm_out[:, h, :], dims, precision=highest,
                    preferred_element_type=jnp.float32,
                )
                kept["norm", h] = carries[h] * jnp.sum(
                    jnp.where(belongs, against, 0.0), axis=1, keepdims=True
                )
        elif c == 1:
            for h in range(heads):
                cols = slice(h * key_width, (h + 1) * key_width)
                scores = decays[h] * lax.dot_general(
                    kept["query"][:, cols], done[:, cols], dims, preferred_element_type=jnp.float32
                )
                den = jnp.sum(scores, axis=1, keepdims=True) + kept["norm", h]
                kept["scores", h] = scores
                kept["den", h] = jnp.maximum(jnp.abs(den), tops[h])
        else:
            wide = min(width, value_width)
            for i in range(width // wide):
                first = (c - 2) * width + i * wide
                h, sub = first // value_width, first % value_width
                scores = kept["scores", h]
                high = scores.astype(jnp.bfloat16)
                low = (scores - high.astype(jnp.float32)).astype(jnp.bfloat16)
                mine = done[:, i * wide : (i + 1) * wide]
                num = carried[h, :, sub : sub + wide]
                num = num + jnp.dot(high, mine, preferred_element_type=jnp.float32)
                num = num + jnp.dot(low, mine, preferred_element_type=jnp.float32)
                result = num / kept["den", h]
                for n in range(seqs):
                    out_ref[n, :, first : first + wide] = result[
                        n * length : (n + 1) * length
                    ].astype(jnp.bfloat16)

    for c in range(chunks + 3):
        if c < chunks:
            if c == 0:
                mem_copy.wait()
            relay(c)
            for h in range(c, heads, 2) if c < 2 else ():
                fold(h)
        if c == 1:
            receive_rows()
        if 1 <= c <= chunks:
            partial(c - 1)
        if c >= 3:
            finish(c - 3)
    for copy in sends[-pool:]:
        copy.wait_send()


def write_kernel(*refs):
    count = (len(refs) - 1) // 2
    sems = refs[-1]
    copies = []
    for src, dst in zip(refs[:count], refs[count : 2 * count]):
        copies.append((src, dst))
    copies = [pltpu.make_async_copy(s, d, sems.at[i]) for i, (s, d) in enumerate(copies)]
    for copy in copies:
        copy.start()
    for copy in copies:
        copy.wait()


def step(
    tokens,
    norm_gain,
    w_query,
    w_key,
    w_value,
    w_igate,
    w_fgate,
    igate_bias,
    fgate_bias,
    prev_keys,
    prev_values,
    prev_igate,
    prev_logf,
    accepted,
    state_mem,
    state_norm,
    state_max,
    kv_n,
    tp_n,
):
    seqs, length, part = tokens.shape
    rows = seqs * length
    heads, key_width, value_width = state_mem.shape[1:]
    depth, width = w_query.shape
    chunks = 2 + w_value.shape[1] // width
    reduce_n, group_n = factor(kv_n)
    outer_n, inner_n = factor(group_n)
    block = group_n * depth
    stride = -(-rows // 16) * 16
    dma = pltpu.SemaphoreType.DMA
    peers = max(1, outer_n + inner_n - 2)
    others = max(1, reduce_n - 1)
    relays = (max(1, inner_n - 1), max(1, outer_n - 1))
    vmem = pl.BlockSpec(memory_space=pltpu.VMEM)
    hbm = pl.BlockSpec(memory_space=pl.ANY)
    small = (
        norm_gain.reshape(1, -1),
        w_igate.T,
        w_fgate.T,
        igate_bias.reshape(1, -1),
        fgate_bias.reshape(1, -1),
        prev_keys,
        prev_values,
        prev_igate.transpose(1, 2, 0),
        prev_logf.transpose(1, 2, 0),
        accepted.reshape(1, -1),
        state_norm,
        state_max.T,
    )
    results = (
        jax.ShapeDtypeStruct((seqs, length, heads * value_width), jnp.bfloat16),
        jax.ShapeDtypeStruct(state_mem.shape, jnp.float32),
        jax.ShapeDtypeStruct(state_norm.shape, jnp.float32),
        jax.ShapeDtypeStruct((heads, seqs), jnp.float32),
    )
    held = pl.pallas_call(
        functools.partial(step_kernel, reduce_n, outer_n, inner_n, tp_n),
        out_shape=results,
        in_specs=[hbm] * (5 + len(small)),
        out_specs=[vmem] * len(results),
        scratch_shapes=[pltpu.VMEM(x.shape, x.dtype) for x in small]
        + [
            pltpu.VMEM((tp_n, seqs, length, part), jnp.bfloat16),
            pltpu.VMEM((tp_n, rows, part), jnp.float32),
            pltpu.VMEM((stride, heads * key_width), jnp.float32),
            pltpu.VMEM((stride, heads * value_width), jnp.float32),
            pltpu.VMEM((heads, 2 * stride, key_width), jnp.float32),
            pltpu.VMEM((heads, seqs * key_width, value_width), jnp.bfloat16),
            pltpu.VMEM((heads, rows, value_width), jnp.float32),
            pltpu.VMEM((reduce_n, rows, block), jnp.bfloat16),
            pltpu.VMEM((others, rows, block), jnp.bfloat16),
            pltpu.VMEM((reduce_n * stride, block), jnp.bfloat16),
            pltpu.VMEM((chunks, block, width), jnp.bfloat16),
            pltpu.VMEM((chunks, rows, width), jnp.float32),
            pltpu.VMEM((chunks, others, rows, width), jnp.bfloat16),
            pltpu.VMEM((chunks, others, rows, width), jnp.bfloat16),
            dma,
            dma((pool,)),
            dma((max(1, tp_n - 1),)),
            dma,
            dma((chunks,)),
            dma((chunks, peers)),
            dma((chunks,) + relays),
            dma((chunks,)),
            dma,
            dma((len(small),)),
            pltpu.SemaphoreType.REGULAR,
            pltpu.SemaphoreType.REGULAR,
        ],
        compiler_params=pltpu.CompilerParams(
            collective_id=0, has_side_effects=True, vmem_limit_bytes=40 * 2**20
        ),
        name="step",
    )(*(pltpu.with_memory_space_constraint(x, pltpu.HBM) for x in (tokens, w_query, w_key, w_value, state_mem) + small))
    return pl.pallas_call(
        write_kernel,
        out_shape=results,
        in_specs=[vmem] * len(results),
        out_specs=[hbm] * len(results),
        scratch_shapes=[dma((seqs + len(results),))],
        compiler_params=pltpu.CompilerParams(vmem_limit_bytes=8 * 2**20),
        name="write",
    )(*held)


def shards(kv_n, tp_n, *args):
    readout, base_mem, base_norm, base_max = step(*args, kv_n, tp_n)
    return (readout, base_mem, base_norm, base_max.T)


def solution(mesh):
    return jax.shard_map(
        functools.partial(shards, mesh.shape["kv"], mesh.shape["tp"]),
        mesh=mesh,
        in_specs=(
            P("kv", None, "tp"),
            P(),
            P("kv", "tp"),
            P("kv", "tp"),
            P("kv", "tp"),
            P(),
            P(),
            P(),
            P(),
            P("kv", None, "tp"),
            P("kv", None, "tp"),
            P("kv", None, "tp"),
            P("kv", None, "tp"),
            P("kv"),
            P("kv", "tp", None, None),
            P("kv", "tp", None),
            P("kv", "tp"),
        ),
        out_specs=(
            P("kv", None, "tp"),
            P("kv", "tp", None, None),
            P("kv", "tp", None),
            P("kv", "tp"),
        ),
        check_vma=False,
    )
```

```python
import functools
import math

import jax
import jax.numpy as jnp
from jax import lax
from jax.experimental import pallas as pl
from jax.experimental.pallas import tpu as pltpu
from jax.sharding import PartitionSpec as P

epsilon = 1e-06
pool = 10
highest = lax.Precision.HIGHEST


def factor(count):
    inner = 1
    while inner * inner * 4 <= count and count % (inner * 2) == 0:
        inner *= 2
    return count // inner, inner


def step_kernel(
    reduce_n,
    outer_n,
    inner_n,
    tp_n,
    turned_chunk,
    tok_ref,
    wq_ref,
    wk_ref,
    wv_ref,
    mem_ref,
    *refs,
):
    small_n = 12
    hbm_small, refs = refs[:small_n], refs[small_n:]
    (out_ref, mem_out, norm_out, max_out), refs = refs[:4], refs[4:]
    vmem_small, refs = refs[:small_n], refs[small_n:]
    (
        gain_ref,
        wi_ref,
        wf_ref,
        bi_ref,
        bf_ref,
        keys_ref,
        values_ref,
        gate_ref,
        logf_ref,
        accepted_ref,
        norm_ref,
        max_ref,
    ) = vmem_small
    (
        xfull,
        xrows,
        krows,
        vrows,
        scaled,
        mem16,
        carried,
        nbuf,
        abuf,
        xall,
        nturn,
        aturn,
        xturn,
        wbuf,
        own,
        sbuf,
        rbuf,
        tok_local,
        send_sem,
        tok_recv,
        a_recv,
        w_local,
        w_recv,
        f_recv,
        p_recv,
        mem_sem,
        small_sem,
        up_sem,
        down_sem,
        side_sem,
        turn_recv,
    ) = refs
    group_n = outer_n * inner_n
    chunks, rows_all, width = wbuf.shape
    depth = rows_all // group_n
    cut = depth * 5 // 128 * 16 if turned_chunk is not None else depth // 2
    seqs, length, part = tok_ref.shape
    rows = seqs * length
    heads, _, value_width = mem16.shape
    key_width = mem_ref.shape[2]
    key_scale = key_width ** (-0.5)
    stride = xall.shape[0] // reduce_n
    block = nbuf.shape[2]

    kv = lax.axis_index("kv")
    tp = lax.axis_index("tp")
    red, grp = kv // group_n, kv % group_n
    outer, inner = grp // inner_n, grp % inner_n

    def at_grp(index):
        return {"kv": red * group_n + index}

    x_peers = [outer * inner_n + (inner + d) % inner_n for d in range(1, inner_n)]
    y_peers = [((outer + d) % outer_n) * inner_n + inner for d in range(1, outer_n)]
    t_peers = [(tp + d) % tp_n for d in range(1, tp_n)]
    x_back = [outer * inner_n + (inner + inner_n - d) % inner_n for d in range(1, inner_n)]
    y_back = [((outer + outer_n - d) % outer_n) * inner_n + inner for d in range(1, outer_n)]
    r_peers = [(red + d) % reduce_n for d in range(1, reduce_n)]
    r_back = [(red + reduce_n - d) % reduce_n for d in range(1, reduce_n)]
    t_back = [(tp + tp_n - d) % tp_n for d in range(1, tp_n)]

    high_n = max(1, reduce_n // 2)
    high, low = red // 2, red % 2
    low_kv = (high * 2 + 1 - low) * group_n + grp
    steps = [(dh, dy) for dh in range(high_n) for dy in range(outer_n)][1:]
    turned_back = [
        ((high + high_n - dh) % high_n, (outer + outer_n - dy) % outer_n) for dh, dy in steps
    ]

    def turned_kv(h, y):
        return {"kv": (h * 2 + low) * group_n + y * inner_n + inner}

    barrier = pltpu.get_barrier_semaphore()
    targets = (
        [{"tp": t} for t in t_peers]
        + [at_grp(p) for p in x_peers + y_peers]
    )

    def signal(sem, target):
        pl.semaphore_signal(sem, inc=1, device_id=target, device_id_type=pl.DeviceIdType.MESH)

    def at_red(index):
        return {"kv": index * group_n + grp}

    for target in targets:
        signal(barrier, target)
    has_below, has_above = red > 0, red < reduce_n - 1
    if reduce_n > 1:
        pl.when(has_below)(lambda: signal(barrier, at_red(red - 1)))
        pl.when(has_above)(lambda: signal(barrier, at_red(red + 1)))

    def chunk_of(c):
        if c == 0:
            return wq_ref
        if c == 1:
            return wk_ref
        return wv_ref.at[:, pl.ds((c - 2) * width, width)]

    def slot(c, source, start=0, size=None):
        size = depth if size is None else size
        first = pl.multiple_of(source * depth + start, math.gcd(depth, start))
        return wbuf.at[c, pl.ds(first, size), :]

    def home(c):
        return low * inner_n + inner if c == turned_chunk else grp

    def remote(src, dst, send, recv, target):
        return pltpu.make_async_remote_copy(
            src_ref=src,
            dst_ref=dst,
            send_sem=send,
            recv_sem=recv,
            device_id=target,
            device_id_type=pl.DeviceIdType.MESH,
        )

    tok_copy = pltpu.make_async_copy(tok_ref, xfull.at[tp], tok_local)
    w_copies = [
        pltpu.make_async_copy(chunk_of(c), slot(c, home(c)), w_local.at[c]) for c in range(chunks)
    ]
    for copy in w_copies[:1] + [tok_copy] + w_copies[1:]:
        copy.start()
    small = [
        pltpu.make_async_copy(src, dst, small_sem.at[i])
        for i, (src, dst) in enumerate(zip(hbm_small, vmem_small))
    ]
    for copy in small:
        copy.start()
    mem_copy = pltpu.make_async_copy(mem_ref, mem_out, mem_sem)
    mem_copy.start()
    greeted = len(targets)
    if reduce_n > 1:
        greeted = greeted + jnp.minimum(red, 1) + jnp.minimum(reduce_n - 1 - red, 1)
    pl.semaphore_wait(barrier, greeted)

    sends = []

    def go(src, dst, recv, target):
        count = len(sends)
        if count >= pool:
            sends[count - pool].wait_send()
        copy = remote(src, dst, send_sem.at[count % pool], recv, target)
        copy.start()
        sends.append(copy)

    def direct(c):
        w_copies[c].wait()
        here = slot(c, home(c))
        second = [{"kv": low_kv}] if c == turned_chunk else [at_grp(p) for p in y_peers]
        for i, target in enumerate([at_grp(p) for p in x_peers] + second):
            go(here, here, w_recv.at[c, i], target)

    direct(0)
    tok_copy.wait()
    for i, t in enumerate(t_peers):
        go(xfull.at[tp], xfull.at[tp], tok_recv.at[i], {"tp": t})
    if chunks > 1:
        direct(1)

    if reduce_n > 2:
        last = reduce_n - 1
        pl.when(red == 1)(lambda: signal(up_sem, at_red(red + 1)))
        pl.when(red == last - 1)(lambda: signal(down_sem, at_red(red - 1)))
        pl.when(red >= 2)(lambda: pl.semaphore_wait(up_sem, 1))
        pl.when((red >= 2) & (red < last))(lambda: signal(up_sem, at_red(red + 1)))
        pl.when(red <= last - 2)(lambda: pl.semaphore_wait(down_sem, 1))
        pl.when((red <= last - 2) & (red > 0))(lambda: signal(down_sem, at_red(red - 1)))

    for i, t in enumerate(t_back):
        remote(xfull.at[t], xfull.at[t], send_sem.at[0], tok_recv.at[i], {"tp": t}).wait_recv()

    small[0].wait()
    total = jnp.zeros((rows, 1), jnp.float32)
    for t in range(tp_n):
        for n in range(seqs):
            xrows[t, n * length : (n + 1) * length] = xfull[t, n].astype(jnp.float32)
        piece = xrows[t]
        total = total + jnp.sum(piece * piece, axis=1, keepdims=True)
    factor_rows = lax.rsqrt(total / (tp_n * part) + epsilon)
    step = min(block, part)
    turned_spots = [
        (h, y, a) for h in range(high_n) for y in range(outer_n) for a in range(2)
    ] if turned_chunk is not None else []
    for p in range(reduce_n * block // step):
        first = p * step
        piece = xrows[first // part, :, first % part : first % part + step]
        normed = (piece * factor_rows * gain_ref[:, first : first + step]).astype(jnp.bfloat16)
        nbuf[first // block, :, first % block : first % block + step] = normed
        for h, y, a in turned_spots:
            begin = ((h * 2 + a) * group_n + y * inner_n) * depth - first
            if 0 <= begin < step:
                run = inner_n * depth
                nturn[h * outer_n + y, :, a * run : (a + 1) * run] = normed[:, begin : begin + run]

    for i, p in enumerate(r_peers):
        go(nbuf.at[p], abuf.at[i], a_recv, {"kv": p * group_n + grp})
    if turned_chunk is not None:
        for dh in range(1, high_n):
            signal(side_sem, turned_kv((high + dh) % high_n, outer))
        if high_n > 1:
            pl.semaphore_wait(side_sem, high_n - 1)
        for i, (dh, dy) in enumerate(steps):
            h, y = (high + dh) % high_n, (outer + dy) % outer_n
            go(nturn.at[h * outer_n + y], aturn.at[i], turn_recv, turned_kv(h, y))

    for copy in small[1:]:
        copy.wait()

    row_seq = lax.broadcasted_iota(jnp.int32, (rows, seqs), 0) // length
    row_pos = lax.broadcasted_iota(jnp.int32, (rows, seqs), 0) % length
    belongs = row_seq == lax.broadcasted_iota(jnp.int32, (rows, seqs), 1)
    diagonal = lax.broadcasted_iota(jnp.int32, (seqs, seqs), 0) == lax.broadcasted_iota(
        jnp.int32, (seqs, seqs), 1
    )

    accepted = accepted_ref[...]
    summed = jnp.zeros((heads, seqs), jnp.float32)
    sums = []
    for j in range(length):
        summed = summed + jnp.where(j < accepted, logf_ref[j], 0.0)
        sums.append(summed)
    logs = [
        jnp.where(j < accepted, summed - sums[j] + gate_ref[j], -jnp.inf) for j in range(length)
    ]
    top_log = summed + max_ref[...]
    for log in logs:
        top_log = jnp.maximum(top_log, log)
    max_out[...] = top_log
    weights = [jnp.exp(log - top_log) for log in logs]
    keep = jnp.exp(summed + max_ref[...] - top_log)

    krows[...] = jnp.zeros_like(krows)
    vrows[...] = jnp.zeros_like(vrows)
    scaled[...] = jnp.zeros_like(scaled)
    for n in range(seqs):
        krows[n * length : (n + 1) * length] = keys_ref[n].astype(jnp.float32)
        vrows[n * length : (n + 1) * length] = values_ref[n].astype(jnp.float32)
    values = vrows[...].astype(jnp.bfloat16)
    values = jnp.concatenate([values, values], axis=0)
    lane_seq = lax.broadcasted_iota(jnp.int32, (key_width, 2 * stride), 1) % stride // length
    pick_seq = (
        lax.broadcasted_iota(jnp.int32, (seqs, 2 * stride), 1) % stride // length
        == lax.broadcasted_iota(jnp.int32, (seqs, 2 * stride), 0)
    ).astype(jnp.bfloat16)

    def fold(h):
        column = jnp.zeros((rows, seqs), jnp.float32)
        for j in range(length):
            column = column + jnp.where(belongs & (row_pos == j), weights[j][h : h + 1], 0.0)
        column = jnp.sum(column, axis=1, keepdims=True)
        keys = krows[:rows, h * key_width : (h + 1) * key_width] * key_scale * column
        high = keys.astype(jnp.bfloat16).astype(jnp.float32)
        scaled[h, :rows] = high
        scaled[h, stride : stride + rows] = keys - high
        block_keys = scaled[h]
        upright = block_keys.T
        mine = values[:, h * value_width : (h + 1) * value_width]
        for n in range(seqs):
            left = jnp.where(lane_seq == n, upright, 0.0).astype(jnp.bfloat16)
            update = jnp.dot(left, mine, preferred_element_type=jnp.float32)
            fresh = keep[h : h + 1, n : n + 1] * mem_out[n, h] + update
            mem_out[n, h] = fresh
            mem16[h, n * key_width : (n + 1) * key_width] = fresh.astype(jnp.bfloat16)
        carry = jnp.sum(jnp.where(diagonal, keep[h : h + 1], 0.0), axis=1, keepdims=True)
        added = jnp.dot(pick_seq, block_keys.astype(jnp.bfloat16), preferred_element_type=jnp.float32)
        norm_out[:, h, :] = carry * norm_ref[:, h, :] + added

    dims = (((1,), (1,)), ((), ()))
    gate_i = jnp.zeros((rows, wi_ref.shape[0]), jnp.float32)
    gate_f = jnp.zeros((rows, wf_ref.shape[0]), jnp.float32)
    for p in range(reduce_n):
        cols = slice(p * block, (p + 1) * block)
        piece = nbuf[p]
        gate_i += lax.dot_general(piece, wi_ref[:, cols], dims, preferred_element_type=jnp.float32)
        gate_f += lax.dot_general(piece, wf_ref[:, cols], dims, preferred_element_type=jnp.float32)
    gate_i = gate_i + bi_ref[...]
    gate_f = jax.nn.log_sigmoid(gate_f + bf_ref[...])
    row_id = lax.broadcasted_iota(jnp.int32, (rows, rows), 0)
    col_id = lax.broadcasted_iota(jnp.int32, (rows, rows), 1)
    causal = (row_id // length == col_id // length) & (col_id <= row_id)
    same = row_id == col_id
    head_id = lax.broadcasted_iota(jnp.int32, gate_i.shape, 1)

    def turned(column):
        return jnp.sum(jnp.where(same, column, 0.0), axis=0, keepdims=True)

    decays, tops, carries = [], [], []
    for h in range(heads):
        chosen = head_id == tp * heads + h
        in_gate = jnp.sum(jnp.where(chosen, gate_i, 0.0), axis=1, keepdims=True)
        log_forget = jnp.sum(jnp.where(chosen, gate_f, 0.0), axis=1, keepdims=True)
        running = jnp.sum(jnp.where(causal, turned(log_forget), 0.0), axis=1, keepdims=True)
        within = jnp.where(causal, running + turned(in_gate - running), -jnp.inf)
        base_max = jnp.sum(jnp.where(belongs, top_log[h : h + 1], 0.0), axis=1, keepdims=True)
        top = jnp.maximum(running + base_max, jnp.max(within, axis=1, keepdims=True))
        decays.append(jnp.exp(within - top) * key_scale)
        carries.append(jnp.exp(running + base_max - top))
        tops.append(jnp.exp(-top))

    def receive_rows():
        xall[...] = jnp.zeros_like(xall)
        xall[:rows, :] = nbuf[red]
        if reduce_n > 1:
            remote(abuf, abuf, send_sem.at[0], a_recv, {"kv": r_back[0] * group_n + grp}).wait_recv()
        for i in range(reduce_n - 1):
            xall[(i + 1) * stride : (i + 1) * stride + rows, :] = abuf[i]

    def relay_turned(c):
        for i, p in enumerate(x_back):
            here = slot(c, low * inner_n + p % inner_n)
            remote(here, here, send_sem.at[0], w_recv.at[c, i], at_grp(p)).wait_recv()
            go(here, here, f_recv.at[c, i, 0], {"kv": low_kv})
        k = len(x_back)
        here = slot(c, (1 - low) * inner_n + inner)
        remote(here, here, send_sem.at[0], w_recv.at[c, k], {"kv": low_kv}).wait_recv()
        if c + 2 < chunks:
            direct(c + 2)

    def relay(c):
        if c == turned_chunk:
            relay_turned(c)
            return
        for i, p in enumerate(x_back):
            remote(slot(c, p), slot(c, p), send_sem.at[0], w_recv.at[c, i], at_grp(p)).wait_recv()
            for j, q in enumerate(y_peers):
                piece = slot(c, p, 0, cut)
                go(piece, piece, f_recv.at[c, i, j], at_grp(q))
        for j, q in enumerate(y_back):
            k = len(x_back) + j
            remote(slot(c, q), slot(c, q), send_sem.at[0], w_recv.at[c, k], at_grp(q)).wait_recv()
            for i, p in enumerate(x_peers):
                piece = slot(c, q, cut, depth - cut)
                go(piece, piece, f_recv.at[c, i, j], at_grp(p))
        if c + 2 < chunks:
            direct(c + 2)

    def receive_turned():
        xturn[...] = jnp.zeros_like(xturn)
        xturn[:rows, :] = nturn[high * outer_n + outer]
        remote(aturn, aturn, send_sem.at[0], turn_recv, turned_kv(*turned_back[0])).wait_recv()
        for i in range(reduce_n - 1):
            xturn[(i + 1) * stride : (i + 1) * stride + rows, :] = aturn[i]

    def land(c):
        for i, p in enumerate(x_back):
            for j, q in enumerate(y_back):
                source = q - inner + p - outer * inner_n
                here = slot(c, source)
                remote(here, here, send_sem.at[0], f_recv.at[c, i, j], at_grp(source)).wait_recv()

    def partial(c):
        rows_in, owners = xall, [at_red(p) for p in r_back]
        if c == turned_chunk:
            rows_in, owners = xturn, [turned_kv(h, y) for h, y in turned_back]
            for i, p in enumerate(x_back):
                here = slot(c, (1 - low) * inner_n + p % inner_n)
                remote(here, here, send_sem.at[0], f_recv.at[c, i, 0], {"kv": low_kv}).wait_recv()
        else:
            land(c)
        product = jnp.dot(rows_in[...], wbuf[c], preferred_element_type=jnp.float32)
        own[c] = product[:rows]
        for i, owner in reversed(list(enumerate(owners))):
            piece = product[(i + 1) * stride : (i + 1) * stride + rows]
            sbuf[c, i] = piece.astype(jnp.bfloat16)
            go(sbuf.at[c, i], rbuf.at[c, i], p_recv.at[c], owner)

    def settle(c):
        total = own[c]
        if reduce_n > 1:
            here = rbuf.at[c]
            source = {"kv": r_back[0] * group_n + grp}
            remote(here, here, send_sem.at[0], p_recv.at[c], source).wait_recv()
        for i in range(reduce_n - 1):
            total = total + rbuf[c, i].astype(jnp.float32)
        return total.astype(jnp.bfloat16)

    kept = {}

    def finish(c):
        done = settle(c)
        if c == 0:
            kept["query"] = done
            seq_id = lax.broadcasted_iota(jnp.int32, (rows, key_width), 0) // length
            for h in range(heads):
                query = done[:, h * key_width : (h + 1) * key_width].astype(jnp.float32)
                spread = jnp.concatenate(
                    [jnp.where(seq_id == n, query, 0.0).astype(jnp.bfloat16) for n in range(seqs)],
                    axis=1,
                )
                held = jnp.dot(spread, mem16[h], preferred_element_type=jnp.float32)
                carried[h] = held * carries[h]
                against = lax.dot_general(
                    query, norm_out[:, h, :], dims, precision=highest,
                    preferred_element_type=jnp.float32,
                )
                kept["norm", h] = carries[h] * jnp.sum(
                    jnp.where(belongs, against, 0.0), axis=1, keepdims=True
                )
        elif c == 1:
            for h in range(heads):
                cols = slice(h * key_width, (h + 1) * key_width)
                scores = decays[h] * lax.dot_general(
                    kept["query"][:, cols], done[:, cols], dims, preferred_element_type=jnp.float32
                )
                den = jnp.sum(scores, axis=1, keepdims=True) + kept["norm", h]
                kept["scores", h] = scores
                kept["den", h] = jnp.maximum(jnp.abs(den), tops[h])
        else:
            wide = min(width, value_width)
            for i in range(width // wide):
                first = (c - 2) * width + i * wide
                h, sub = first // value_width, first % value_width
                scores = kept["scores", h]
                high = scores.astype(jnp.bfloat16)
                low = (scores - high.astype(jnp.float32)).astype(jnp.bfloat16)
                mine = done[:, i * wide : (i + 1) * wide]
                num = carried[h, :, sub : sub + wide]
                num = num + jnp.dot(high, mine, preferred_element_type=jnp.float32)
                num = num + jnp.dot(low, mine, preferred_element_type=jnp.float32)
                result = num / kept["den", h]
                for n in range(seqs):
                    out_ref[n, :, first : first + wide] = result[
                        n * length : (n + 1) * length
                    ].astype(jnp.bfloat16)

    for c in range(chunks + 3):
        if c < chunks:
            if c == 0:
                mem_copy.wait()
            relay(c)
            for h in range(c, heads, 2) if c < 2 else ():
                fold(h)
        if c == 1:
            receive_rows()
            if turned_chunk is not None:
                receive_turned()
        if 1 <= c <= chunks:
            partial(c - 1)
        if c >= 3:
            finish(c - 3)
    for copy in sends[-pool:]:
        copy.wait_send()


def write_kernel(*refs):
    count = (len(refs) - 1) // 2
    sems = refs[-1]
    copies = []
    for src, dst in zip(refs[:count], refs[count : 2 * count]):
        copies.append((src, dst))
    copies = [pltpu.make_async_copy(s, d, sems.at[i]) for i, (s, d) in enumerate(copies)]
    for copy in copies:
        copy.start()
    for copy in copies:
        copy.wait()


def step(
    tokens,
    norm_gain,
    w_query,
    w_key,
    w_value,
    w_igate,
    w_fgate,
    igate_bias,
    fgate_bias,
    prev_keys,
    prev_values,
    prev_igate,
    prev_logf,
    accepted,
    state_mem,
    state_norm,
    state_max,
    kv_n,
    tp_n,
):
    seqs, length, part = tokens.shape
    rows = seqs * length
    heads, key_width, value_width = state_mem.shape[1:]
    depth, width = w_query.shape
    chunks = 2 + w_value.shape[1] // width
    reduce_n, group_n = factor(kv_n)
    outer_n, inner_n = factor(group_n)
    block = group_n * depth
    stride = -(-rows // 16) * 16
    dma = pltpu.SemaphoreType.DMA
    peers = max(1, outer_n + inner_n - 2)
    square = outer_n == 2 and inner_n == 2 and reduce_n == 4 and (depth * inner_n) % 128 == 0
    turned_chunk = 2 if square else None
    others = max(1, reduce_n - 1)
    relays = (max(1, inner_n - 1), max(1, outer_n - 1))
    vmem = pl.BlockSpec(memory_space=pltpu.VMEM)
    hbm = pl.BlockSpec(memory_space=pl.ANY)
    small = (
        norm_gain.reshape(1, -1),
        w_igate.T,
        w_fgate.T,
        igate_bias.reshape(1, -1),
        fgate_bias.reshape(1, -1),
        prev_keys,
        prev_values,
        prev_igate.transpose(1, 2, 0),
        prev_logf.transpose(1, 2, 0),
        accepted.reshape(1, -1),
        state_norm,
        state_max.T,
    )
    results = (
        jax.ShapeDtypeStruct((seqs, length, heads * value_width), jnp.bfloat16),
        jax.ShapeDtypeStruct(state_mem.shape, jnp.float32),
        jax.ShapeDtypeStruct(state_norm.shape, jnp.float32),
        jax.ShapeDtypeStruct((heads, seqs), jnp.float32),
    )
    held = pl.pallas_call(
        functools.partial(step_kernel, reduce_n, outer_n, inner_n, tp_n, turned_chunk),
        out_shape=results,
        in_specs=[hbm] * (5 + len(small)),
        out_specs=[vmem] * len(results),
        scratch_shapes=[pltpu.VMEM(x.shape, x.dtype) for x in small]
        + [
            pltpu.VMEM((tp_n, seqs, length, part), jnp.bfloat16),
            pltpu.VMEM((tp_n, rows, part), jnp.float32),
            pltpu.VMEM((stride, heads * key_width), jnp.float32),
            pltpu.VMEM((stride, heads * value_width), jnp.float32),
            pltpu.VMEM((heads, 2 * stride, key_width), jnp.float32),
            pltpu.VMEM((heads, seqs * key_width, value_width), jnp.bfloat16),
            pltpu.VMEM((heads, rows, value_width), jnp.float32),
            pltpu.VMEM((reduce_n, rows, block), jnp.bfloat16),
            pltpu.VMEM((others, rows, block), jnp.bfloat16),
            pltpu.VMEM((reduce_n * stride, block), jnp.bfloat16),
            pltpu.VMEM((reduce_n, rows, block), jnp.bfloat16),
            pltpu.VMEM((others, rows, block), jnp.bfloat16),
            pltpu.VMEM((reduce_n * stride, block), jnp.bfloat16),
            pltpu.VMEM((chunks, block, width), jnp.bfloat16),
            pltpu.VMEM((chunks, rows, width), jnp.float32),
            pltpu.VMEM((chunks, others, rows, width), jnp.bfloat16),
            pltpu.VMEM((chunks, others, rows, width), jnp.bfloat16),
            dma,
            dma((pool,)),
            dma((max(1, tp_n - 1),)),
            dma,
            dma((chunks,)),
            dma((chunks, peers)),
            dma((chunks,) + relays),
            dma((chunks,)),
            dma,
            dma((len(small),)),
            pltpu.SemaphoreType.REGULAR,
            pltpu.SemaphoreType.REGULAR,
            pltpu.SemaphoreType.REGULAR,
            dma,
        ],
        compiler_params=pltpu.CompilerParams(
            collective_id=0, has_side_effects=True, vmem_limit_bytes=40 * 2**20
        ),
        name="step",
    )(*(pltpu.with_memory_space_constraint(x, pltpu.HBM) for x in (tokens, w_query, w_key, w_value, state_mem) + small))
    return pl.pallas_call(
        write_kernel,
        out_shape=results,
        in_specs=[vmem] * len(results),
        out_specs=[hbm] * len(results),
        scratch_shapes=[dma((seqs + len(results),))],
        compiler_params=pltpu.CompilerParams(vmem_limit_bytes=8 * 2**20),
        name="write",
    )(*held)


def shards(kv_n, tp_n, *args):
    readout, base_mem, base_norm, base_max = step(*args, kv_n, tp_n)
    return (readout, base_mem, base_norm, base_max.T)


def solution(mesh):
    return jax.shard_map(
        functools.partial(shards, mesh.shape["kv"], mesh.shape["tp"]),
        mesh=mesh,
        in_specs=(
            P("kv", None, "tp"),
            P(),
            P("kv", "tp"),
            P("kv", "tp"),
            P("kv", "tp"),
            P(),
            P(),
            P(),
            P(),
            P("kv", None, "tp"),
            P("kv", None, "tp"),
            P("kv", None, "tp"),
            P("kv", None, "tp"),
            P("kv"),
            P("kv", "tp", None, None),
            P("kv", "tp", None),
            P("kv", "tp"),
        ),
        out_specs=(
            P("kv", None, "tp"),
            P("kv", "tp", None, None),
            P("kv", "tp", None),
            P("kv", "tp"),
        ),
        check_vma=False,
    )
```

```python
import functools
import math

import jax
import jax.numpy as jnp
from jax import lax
from jax.experimental import pallas as pl
from jax.experimental.pallas import tpu as pltpu
from jax.sharding import PartitionSpec as P

epsilon = 1e-06
pool = 6
highest = lax.Precision.HIGHEST


def factor(count):
    inner = 1
    while inner * inner * 4 <= count and count % (inner * 2) == 0:
        inner *= 2
    return count // inner, inner


def step_kernel(
    reduce_n,
    outer_n,
    inner_n,
    tp_n,
    turned_chunk,
    tok_ref,
    wq_ref,
    wk_ref,
    wv_ref,
    mem_ref,
    *refs,
):
    small_n = 12
    hbm_small, refs = refs[:small_n], refs[small_n:]
    (out_ref, mem_out, norm_out, max_out), refs = refs[:4], refs[4:]
    vmem_small, refs = refs[:small_n], refs[small_n:]
    (
        gain_ref,
        wi_ref,
        wf_ref,
        bi_ref,
        bf_ref,
        keys_ref,
        values_ref,
        gate_ref,
        logf_ref,
        accepted_ref,
        norm_ref,
        max_ref,
    ) = vmem_small
    (
        xfull,
        xrows,
        krows,
        vrows,
        scaled,
        mem16,
        carried,
        nbuf,
        abuf,
        xall,
        nturn,
        aturn,
        xturn,
        wbuf,
        own,
        sbuf,
        rbuf,
        tok_local,
        send_sem,
        tok_recv,
        a_recv,
        w_local,
        w_recv,
        f_recv,
        p_recv,
        mem_sem,
        small_sem,
        up_sem,
        down_sem,
        side_sem,
        turn_recv,
    ) = refs
    group_n = outer_n * inner_n
    chunks, rows_all, width = wbuf.shape
    depth = rows_all // group_n
    cut = depth * 5 // 128 * 16 if turned_chunk is not None else depth // 2
    seqs, length, part = tok_ref.shape
    rows = seqs * length
    heads, _, value_width = mem16.shape
    key_width = mem_ref.shape[2]
    key_scale = key_width ** (-0.5)
    stride = xall.shape[0] // reduce_n
    block = nbuf.shape[2]

    kv = lax.axis_index("kv")
    tp = lax.axis_index("tp")
    red, grp = kv // group_n, kv % group_n
    outer, inner = grp // inner_n, grp % inner_n

    def at_grp(index):
        return {"kv": red * group_n + index}

    x_peers = [outer * inner_n + (inner + d) % inner_n for d in range(1, inner_n)]
    y_peers = [((outer + d) % outer_n) * inner_n + inner for d in range(1, outer_n)]
    t_peers = [(tp + d) % tp_n for d in range(1, tp_n)]
    x_back = [outer * inner_n + (inner + inner_n - d) % inner_n for d in range(1, inner_n)]
    y_back = [((outer + outer_n - d) % outer_n) * inner_n + inner for d in range(1, outer_n)]
    r_peers = [(red + d) % reduce_n for d in range(1, reduce_n)]
    r_back = [(red + reduce_n - d) % reduce_n for d in range(1, reduce_n)]
    t_back = [(tp + tp_n - d) % tp_n for d in range(1, tp_n)]

    high_n = max(1, reduce_n // 2)
    high, low = red // 2, red % 2
    low_kv = (high * 2 + 1 - low) * group_n + grp
    steps = [(dh, dy) for dh in range(high_n) for dy in range(outer_n)][1:]
    turned_back = [
        ((high + high_n - dh) % high_n, (outer + outer_n - dy) % outer_n) for dh, dy in steps
    ]

    def turned_kv(h, y):
        return {"kv": (h * 2 + low) * group_n + y * inner_n + inner}

    barrier = pltpu.get_barrier_semaphore()
    targets = (
        [{"tp": t} for t in t_peers]
        + [at_grp(p) for p in x_peers + y_peers]
    )

    def signal(sem, target):
        pl.semaphore_signal(sem, inc=1, device_id=target, device_id_type=pl.DeviceIdType.MESH)

    def at_red(index):
        return {"kv": index * group_n + grp}

    for target in targets:
        signal(barrier, target)
    has_below, has_above = red > 0, red < reduce_n - 1
    if reduce_n > 1:
        pl.when(has_below)(lambda: signal(barrier, at_red(red - 1)))
        pl.when(has_above)(lambda: signal(barrier, at_red(red + 1)))

    def chunk_of(c):
        if c == 0:
            return wq_ref
        if c == 1:
            return wk_ref
        return wv_ref.at[:, pl.ds((c - 2) * width, width)]

    def slot(c, source, start=0, size=None):
        size = depth if size is None else size
        first = pl.multiple_of(source * depth + start, math.gcd(depth, start))
        return wbuf.at[c, pl.ds(first, size), :]

    def home(c):
        return low * inner_n + inner if c == turned_chunk else grp

    def remote(src, dst, send, recv, target):
        return pltpu.make_async_remote_copy(
            src_ref=src,
            dst_ref=dst,
            send_sem=send,
            recv_sem=recv,
            device_id=target,
            device_id_type=pl.DeviceIdType.MESH,
        )

    tok_copy = pltpu.make_async_copy(tok_ref, xfull.at[tp], tok_local)
    w_copies = [
        pltpu.make_async_copy(chunk_of(c), slot(c, home(c)), w_local.at[c]) for c in range(chunks)
    ]
    for copy in w_copies[:1] + [tok_copy] + w_copies[1:]:
        copy.start()
    small = [
        pltpu.make_async_copy(src, dst, small_sem.at[i])
        for i, (src, dst) in enumerate(zip(hbm_small, vmem_small))
    ]
    for copy in small:
        copy.start()
    mem_copy = pltpu.make_async_copy(mem_ref, mem_out, mem_sem)
    mem_copy.start()
    greeted = len(targets)
    if reduce_n > 1:
        greeted = greeted + jnp.minimum(red, 1) + jnp.minimum(reduce_n - 1 - red, 1)
    pl.semaphore_wait(barrier, greeted)

    sends = []

    def go(src, dst, recv, target):
        count = len(sends)
        if count >= pool:
            sends[count - pool].wait_send()
        copy = remote(src, dst, send_sem.at[count % pool], recv, target)
        copy.start()
        sends.append(copy)

    def direct(c):
        w_copies[c].wait()
        here = slot(c, home(c))
        second = [{"kv": low_kv}] if c == turned_chunk else [at_grp(p) for p in y_peers]
        for i, target in enumerate([at_grp(p) for p in x_peers] + second):
            go(here, here, w_recv.at[c, i], target)

    direct(0)
    tok_copy.wait()
    for i, t in enumerate(t_peers):
        go(xfull.at[tp], xfull.at[tp], tok_recv.at[i], {"tp": t})
    if chunks > 1:
        direct(1)

    if reduce_n > 2:
        last = reduce_n - 1
        pl.when(red == 1)(lambda: signal(up_sem, at_red(red + 1)))
        pl.when(red == last - 1)(lambda: signal(down_sem, at_red(red - 1)))
        pl.when(red >= 2)(lambda: pl.semaphore_wait(up_sem, 1))
        pl.when((red >= 2) & (red < last))(lambda: signal(up_sem, at_red(red + 1)))
        pl.when(red <= last - 2)(lambda: pl.semaphore_wait(down_sem, 1))
        pl.when((red <= last - 2) & (red > 0))(lambda: signal(down_sem, at_red(red - 1)))

    for i, t in enumerate(t_back):
        remote(xfull.at[t], xfull.at[t], send_sem.at[0], tok_recv.at[i], {"tp": t}).wait_recv()

    small[0].wait()
    total = jnp.zeros((rows, 1), jnp.float32)
    for t in range(tp_n):
        for n in range(seqs):
            xrows[t, n * length : (n + 1) * length] = xfull[t, n].astype(jnp.float32)
        piece = xrows[t]
        total = total + jnp.sum(piece * piece, axis=1, keepdims=True)
    factor_rows = lax.rsqrt(total / (tp_n * part) + epsilon)
    step = min(block, part)
    turned_spots = [
        (h, y, a) for h in range(high_n) for y in range(outer_n) for a in range(2)
    ] if turned_chunk is not None else []
    for p in range(reduce_n * block // step):
        first = p * step
        piece = xrows[first // part, :, first % part : first % part + step]
        normed = (piece * factor_rows * gain_ref[:, first : first + step]).astype(jnp.bfloat16)
        nbuf[first // block, :, first % block : first % block + step] = normed
        for h, y, a in turned_spots:
            begin = ((h * 2 + a) * group_n + y * inner_n) * depth - first
            if 0 <= begin < step:
                run = inner_n * depth
                nturn[h * outer_n + y, :, a * run : (a + 1) * run] = normed[:, begin : begin + run]

    for i, p in enumerate(r_peers):
        go(nbuf.at[p], abuf.at[i], a_recv, {"kv": p * group_n + grp})

    for copy in small[1:]:
        copy.wait()

    row_seq = lax.broadcasted_iota(jnp.int32, (rows, seqs), 0) // length
    row_pos = lax.broadcasted_iota(jnp.int32, (rows, seqs), 0) % length
    belongs = row_seq == lax.broadcasted_iota(jnp.int32, (rows, seqs), 1)
    diagonal = lax.broadcasted_iota(jnp.int32, (seqs, seqs), 0) == lax.broadcasted_iota(
        jnp.int32, (seqs, seqs), 1
    )

    accepted = accepted_ref[...]
    summed = jnp.zeros((heads, seqs), jnp.float32)
    sums = []
    for j in range(length):
        summed = summed + jnp.where(j < accepted, logf_ref[j], 0.0)
        sums.append(summed)
    logs = [
        jnp.where(j < accepted, summed - sums[j] + gate_ref[j], -jnp.inf) for j in range(length)
    ]
    top_log = summed + max_ref[...]
    for log in logs:
        top_log = jnp.maximum(top_log, log)
    max_out[...] = top_log
    weights = [jnp.exp(log - top_log) for log in logs]
    keep = jnp.exp(summed + max_ref[...] - top_log)

    krows[...] = jnp.zeros_like(krows)
    vrows[...] = jnp.zeros_like(vrows)
    scaled[...] = jnp.zeros_like(scaled)
    for n in range(seqs):
        krows[n * length : (n + 1) * length] = keys_ref[n].astype(jnp.float32)
        vrows[n * length : (n + 1) * length] = values_ref[n].astype(jnp.float32)
    values = vrows[...].astype(jnp.bfloat16)
    values = jnp.concatenate([values, values], axis=0)
    lane_seq = lax.broadcasted_iota(jnp.int32, (key_width, 2 * stride), 1) % stride // length
    pick_seq = (
        lax.broadcasted_iota(jnp.int32, (seqs, 2 * stride), 1) % stride // length
        == lax.broadcasted_iota(jnp.int32, (seqs, 2 * stride), 0)
    ).astype(jnp.bfloat16)

    def fold(h):
        column = jnp.zeros((rows, seqs), jnp.float32)
        for j in range(length):
            column = column + jnp.where(belongs & (row_pos == j), weights[j][h : h + 1], 0.0)
        column = jnp.sum(column, axis=1, keepdims=True)
        keys = krows[:rows, h * key_width : (h + 1) * key_width] * key_scale * column
        high = keys.astype(jnp.bfloat16).astype(jnp.float32)
        scaled[h, :rows] = high
        scaled[h, stride : stride + rows] = keys - high
        block_keys = scaled[h]
        upright = block_keys.T
        mine = values[:, h * value_width : (h + 1) * value_width]
        for n in range(seqs):
            left = jnp.where(lane_seq == n, upright, 0.0).astype(jnp.bfloat16)
            update = jnp.dot(left, mine, preferred_element_type=jnp.float32)
            fresh = keep[h : h + 1, n : n + 1] * mem_out[n, h] + update
            mem_out[n, h] = fresh
            mem16[h, n * key_width : (n + 1) * key_width] = fresh.astype(jnp.bfloat16)
        carry = jnp.sum(jnp.where(diagonal, keep[h : h + 1], 0.0), axis=1, keepdims=True)
        added = jnp.dot(pick_seq, block_keys.astype(jnp.bfloat16), preferred_element_type=jnp.float32)
        norm_out[:, h, :] = carry * norm_ref[:, h, :] + added

    dims = (((1,), (1,)), ((), ()))
    gate_i = jnp.zeros((rows, wi_ref.shape[0]), jnp.float32)
    gate_f = jnp.zeros((rows, wf_ref.shape[0]), jnp.float32)
    for p in range(reduce_n):
        cols = slice(p * block, (p + 1) * block)
        piece = nbuf[p]
        gate_i += lax.dot_general(piece, wi_ref[:, cols], dims, preferred_element_type=jnp.float32)
        gate_f += lax.dot_general(piece, wf_ref[:, cols], dims, preferred_element_type=jnp.float32)
    gate_i = gate_i + bi_ref[...]
    gate_f = jax.nn.log_sigmoid(gate_f + bf_ref[...])
    row_id = lax.broadcasted_iota(jnp.int32, (rows, rows), 0)
    col_id = lax.broadcasted_iota(jnp.int32, (rows, rows), 1)
    causal = (row_id // length == col_id // length) & (col_id <= row_id)
    same = row_id == col_id
    head_id = lax.broadcasted_iota(jnp.int32, gate_i.shape, 1)

    def turned(column):
        return jnp.sum(jnp.where(same, column, 0.0), axis=0, keepdims=True)

    decays, tops, carries = [], [], []
    for h in range(heads):
        chosen = head_id == tp * heads + h
        in_gate = jnp.sum(jnp.where(chosen, gate_i, 0.0), axis=1, keepdims=True)
        log_forget = jnp.sum(jnp.where(chosen, gate_f, 0.0), axis=1, keepdims=True)
        running = jnp.sum(jnp.where(causal, turned(log_forget), 0.0), axis=1, keepdims=True)
        within = jnp.where(causal, running + turned(in_gate - running), -jnp.inf)
        base_max = jnp.sum(jnp.where(belongs, top_log[h : h + 1], 0.0), axis=1, keepdims=True)
        top = jnp.maximum(running + base_max, jnp.max(within, axis=1, keepdims=True))
        decays.append(jnp.exp(within - top) * key_scale)
        carries.append(jnp.exp(running + base_max - top))
        tops.append(jnp.exp(-top))

    def receive_rows():
        xall[...] = jnp.zeros_like(xall)
        xall[:rows, :] = nbuf[red]
        if reduce_n > 1:
            remote(abuf, abuf, send_sem.at[0], a_recv, {"kv": r_back[0] * group_n + grp}).wait_recv()
        for i in range(reduce_n - 1):
            xall[(i + 1) * stride : (i + 1) * stride + rows, :] = abuf[i]

    def relay_turned(c):
        for i, p in enumerate(x_back):
            here = slot(c, low * inner_n + p % inner_n)
            remote(here, here, send_sem.at[0], w_recv.at[c, i], at_grp(p)).wait_recv()
            go(here, here, f_recv.at[c, i, 0], {"kv": low_kv})
        k = len(x_back)
        here = slot(c, (1 - low) * inner_n + inner)
        remote(here, here, send_sem.at[0], w_recv.at[c, k], {"kv": low_kv}).wait_recv()
        if c + 2 < chunks:
            direct(c + 2)

    def relay(c):
        if c == turned_chunk:
            relay_turned(c)
            return
        for i, p in enumerate(x_back):
            remote(slot(c, p), slot(c, p), send_sem.at[0], w_recv.at[c, i], at_grp(p)).wait_recv()
            for j, q in enumerate(y_peers):
                piece = slot(c, p, 0, cut)
                go(piece, piece, f_recv.at[c, i, j], at_grp(q))
        for j, q in enumerate(y_back):
            k = len(x_back) + j
            remote(slot(c, q), slot(c, q), send_sem.at[0], w_recv.at[c, k], at_grp(q)).wait_recv()
            for i, p in enumerate(x_peers):
                piece = slot(c, q, cut, depth - cut)
                go(piece, piece, f_recv.at[c, i, j], at_grp(p))
        if c + 2 < chunks:
            direct(c + 2)

    def send_turned():
        for dh in range(1, high_n):
            signal(side_sem, turned_kv((high + dh) % high_n, outer))
        if high_n > 1:
            pl.semaphore_wait(side_sem, high_n - 1)
        for i, (dh, dy) in enumerate(steps):
            h, y = (high + dh) % high_n, (outer + dy) % outer_n
            go(nturn.at[h * outer_n + y], aturn.at[i], turn_recv, turned_kv(h, y))

    def receive_turned():
        xturn[...] = jnp.zeros_like(xturn)
        xturn[:rows, :] = nturn[high * outer_n + outer]
        remote(aturn, aturn, send_sem.at[0], turn_recv, turned_kv(*turned_back[0])).wait_recv()
        for i in range(reduce_n - 1):
            xturn[(i + 1) * stride : (i + 1) * stride + rows, :] = aturn[i]

    def land(c):
        for i, p in enumerate(x_back):
            for j, q in enumerate(y_back):
                source = q - inner + p - outer * inner_n
                here = slot(c, source)
                remote(here, here, send_sem.at[0], f_recv.at[c, i, j], at_grp(source)).wait_recv()

    def partial(c):
        rows_in, owners = xall, [at_red(p) for p in r_back]
        if c == turned_chunk:
            rows_in, owners = xturn, [turned_kv(h, y) for h, y in turned_back]
            for i, p in enumerate(x_back):
                here = slot(c, (1 - low) * inner_n + p % inner_n)
                remote(here, here, send_sem.at[0], f_recv.at[c, i, 0], {"kv": low_kv}).wait_recv()
        else:
            land(c)
        product = jnp.dot(rows_in[...], wbuf[c], preferred_element_type=jnp.float32)
        own[c] = product[:rows]
        for i, owner in reversed(list(enumerate(owners))):
            piece = product[(i + 1) * stride : (i + 1) * stride + rows]
            sbuf[c, i] = piece.astype(jnp.bfloat16)
            go(sbuf.at[c, i], rbuf.at[c, i], p_recv.at[c], owner)

    def settle(c):
        total = own[c]
        if reduce_n > 1:
            here = rbuf.at[c]
            source = {"kv": r_back[0] * group_n + grp}
            remote(here, here, send_sem.at[0], p_recv.at[c], source).wait_recv()
        for i in range(reduce_n - 1):
            total = total + rbuf[c, i].astype(jnp.float32)
        return total.astype(jnp.bfloat16)

    kept = {}

    def finish(c):
        done = settle(c)
        if c == 0:
            kept["query"] = done
            seq_id = lax.broadcasted_iota(jnp.int32, (rows, key_width), 0) // length
            for h in range(heads):
                query = done[:, h * key_width : (h + 1) * key_width].astype(jnp.float32)
                spread = jnp.concatenate(
                    [jnp.where(seq_id == n, query, 0.0).astype(jnp.bfloat16) for n in range(seqs)],
                    axis=1,
                )
                held = jnp.dot(spread, mem16[h], preferred_element_type=jnp.float32)
                carried[h] = held * carries[h]
                against = lax.dot_general(
                    query, norm_out[:, h, :], dims, precision=highest,
                    preferred_element_type=jnp.float32,
                )
                kept["norm", h] = carries[h] * jnp.sum(
                    jnp.where(belongs, against, 0.0), axis=1, keepdims=True
                )
        elif c == 1:
            for h in range(heads):
                cols = slice(h * key_width, (h + 1) * key_width)
                scores = decays[h] * lax.dot_general(
                    kept["query"][:, cols], done[:, cols], dims, preferred_element_type=jnp.float32
                )
                den = jnp.sum(scores, axis=1, keepdims=True) + kept["norm", h]
                kept["scores", h] = scores
                kept["den", h] = jnp.maximum(jnp.abs(den), tops[h])
        else:
            wide = min(width, value_width)
            for i in range(width // wide):
                first = (c - 2) * width + i * wide
                h, sub = first // value_width, first % value_width
                scores = kept["scores", h]
                high = scores.astype(jnp.bfloat16)
                low = (scores - high.astype(jnp.float32)).astype(jnp.bfloat16)
                mine = done[:, i * wide : (i + 1) * wide]
                num = carried[h, :, sub : sub + wide]
                num = num + jnp.dot(high, mine, preferred_element_type=jnp.float32)
                num = num + jnp.dot(low, mine, preferred_element_type=jnp.float32)
                result = num / kept["den", h]
                for n in range(seqs):
                    out_ref[n, :, first : first + wide] = result[
                        n * length : (n + 1) * length
                    ].astype(jnp.bfloat16)

    for c in range(chunks + 3):
        if c < chunks:
            if c == 0:
                mem_copy.wait()
            relay(c)
            if c == 0 and turned_chunk is not None:
                send_turned()
            for h in range(c, heads, 2) if c < 2 else ():
                fold(h)
        if c == 1:
            receive_rows()
        if c == 3 and turned_chunk is not None:
            receive_turned()
        if c == 3:
            finish(0)
        if 1 <= c <= chunks:
            partial(c - 1)
        if c > 3:
            finish(c - 3)
    for copy in sends[-pool:]:
        copy.wait_send()


def write_kernel(*refs):
    count = (len(refs) - 1) // 2
    sems = refs[-1]
    copies = []
    for src, dst in zip(refs[:count], refs[count : 2 * count]):
        copies.append((src, dst))
    copies = [pltpu.make_async_copy(s, d, sems.at[i]) for i, (s, d) in enumerate(copies)]
    for copy in copies:
        copy.start()
    for copy in copies:
        copy.wait()


def step(
    tokens,
    norm_gain,
    w_query,
    w_key,
    w_value,
    w_igate,
    w_fgate,
    igate_bias,
    fgate_bias,
    prev_keys,
    prev_values,
    prev_igate,
    prev_logf,
    accepted,
    state_mem,
    state_norm,
    state_max,
    kv_n,
    tp_n,
):
    seqs, length, part = tokens.shape
    rows = seqs * length
    heads, key_width, value_width = state_mem.shape[1:]
    depth, width = w_query.shape
    chunks = 2 + w_value.shape[1] // width
    reduce_n, group_n = factor(kv_n)
    outer_n, inner_n = factor(group_n)
    block = group_n * depth
    stride = -(-rows // 16) * 16
    dma = pltpu.SemaphoreType.DMA
    peers = max(1, outer_n + inner_n - 2)
    square = outer_n == 2 and inner_n == 2 and reduce_n == 4 and (depth * inner_n) % 128 == 0
    turned_chunk = 2 if square else None
    others = max(1, reduce_n - 1)
    relays = (max(1, inner_n - 1), max(1, outer_n - 1))
    vmem = pl.BlockSpec(memory_space=pltpu.VMEM)
    hbm = pl.BlockSpec(memory_space=pl.ANY)
    small = (
        norm_gain.reshape(1, -1),
        w_igate.T,
        w_fgate.T,
        igate_bias.reshape(1, -1),
        fgate_bias.reshape(1, -1),
        prev_keys,
        prev_values,
        prev_igate.transpose(1, 2, 0),
        prev_logf.transpose(1, 2, 0),
        accepted.reshape(1, -1),
        state_norm,
        state_max.T,
    )
    results = (
        jax.ShapeDtypeStruct((seqs, length, heads * value_width), jnp.bfloat16),
        jax.ShapeDtypeStruct(state_mem.shape, jnp.float32),
        jax.ShapeDtypeStruct(state_norm.shape, jnp.float32),
        jax.ShapeDtypeStruct((heads, seqs), jnp.float32),
    )
    held = pl.pallas_call(
        functools.partial(step_kernel, reduce_n, outer_n, inner_n, tp_n, turned_chunk),
        out_shape=results,
        in_specs=[hbm] * (5 + len(small)),
        out_specs=[vmem] * len(results),
        scratch_shapes=[pltpu.VMEM(x.shape, x.dtype) for x in small]
        + [
            pltpu.VMEM((tp_n, seqs, length, part), jnp.bfloat16),
            pltpu.VMEM((tp_n, rows, part), jnp.float32),
            pltpu.VMEM((stride, heads * key_width), jnp.float32),
            pltpu.VMEM((stride, heads * value_width), jnp.float32),
            pltpu.VMEM((heads, 2 * stride, key_width), jnp.float32),
            pltpu.VMEM((heads, seqs * key_width, value_width), jnp.bfloat16),
            pltpu.VMEM((heads, rows, value_width), jnp.float32),
            pltpu.VMEM((reduce_n, rows, block), jnp.bfloat16),
            pltpu.VMEM((others, rows, block), jnp.bfloat16),
            pltpu.VMEM((reduce_n * stride, block), jnp.bfloat16),
            pltpu.VMEM((reduce_n, rows, block), jnp.bfloat16),
            pltpu.VMEM((others, rows, block), jnp.bfloat16),
            pltpu.VMEM((reduce_n * stride, block), jnp.bfloat16),
            pltpu.VMEM((chunks, block, width), jnp.bfloat16),
            pltpu.VMEM((chunks, rows, width), jnp.float32),
            pltpu.VMEM((chunks, others, rows, width), jnp.bfloat16),
            pltpu.VMEM((chunks, others, rows, width), jnp.bfloat16),
            dma,
            dma((pool,)),
            dma((max(1, tp_n - 1),)),
            dma,
            dma((chunks,)),
            dma((chunks, peers)),
            dma((chunks,) + relays),
            dma((chunks,)),
            dma,
            dma((len(small),)),
            pltpu.SemaphoreType.REGULAR,
            pltpu.SemaphoreType.REGULAR,
            pltpu.SemaphoreType.REGULAR,
            dma,
        ],
        compiler_params=pltpu.CompilerParams(
            collective_id=0, has_side_effects=True, vmem_limit_bytes=40 * 2**20
        ),
        name="step",
    )(*(pltpu.with_memory_space_constraint(x, pltpu.HBM) for x in (tokens, w_query, w_key, w_value, state_mem) + small))
    return pl.pallas_call(
        write_kernel,
        out_shape=results,
        in_specs=[vmem] * len(results),
        out_specs=[hbm] * len(results),
        scratch_shapes=[dma((seqs + len(results),))],
        compiler_params=pltpu.CompilerParams(vmem_limit_bytes=8 * 2**20),
        name="write",
    )(*held)


def shards(kv_n, tp_n, *args):
    readout, base_mem, base_norm, base_max = step(*args, kv_n, tp_n)
    return (readout, base_mem, base_norm, base_max.T)


def solution(mesh):
    return jax.shard_map(
        functools.partial(shards, mesh.shape["kv"], mesh.shape["tp"]),
        mesh=mesh,
        in_specs=(
            P("kv", None, "tp"),
            P(),
            P("kv", "tp"),
            P("kv", "tp"),
            P("kv", "tp"),
            P(),
            P(),
            P(),
            P(),
            P("kv", None, "tp"),
            P("kv", None, "tp"),
            P("kv", None, "tp"),
            P("kv", None, "tp"),
            P("kv"),
            P("kv", "tp", None, None),
            P("kv", "tp", None),
            P("kv", "tp"),
        ),
        out_specs=(
            P("kv", None, "tp"),
            P("kv", "tp", None, None),
            P("kv", "tp", None),
            P("kv", "tp"),
        ),
        check_vma=False,
    )
```
